32 devices in a mesh: ep: 16 (over z, y, x), tp: 2 (over core).
Axes of the slice: x: 2, y: 2, z: 4, core: 2. Of those that a mesh axis runs over, the one named last changes fastest.
Arguments:
- tokens: bfloat16 [256, 2048], P(('ep', 'tp')), may hold values from -6 to 6
- mix_gain: float32 [2048], replicated, may hold values from 0.1 to 1.9
- w_query: bfloat16 [2048, 16, 128], P(None, 'tp', 'ep'), may hold values from -0.125 to 0.125
- w_key: bfloat16 [2048, 16, 128], P(None, 'tp', 'ep'), may hold values from -0.125 to 0.125
- w_value: bfloat16 [2048, 16, 128], P(None, 'tp', 'ep'), may hold values from -0.125 to 0.125
- w_zgate: bfloat16 [2048, 16, 128], P(None, 'tp', 'ep'), may hold values from -0.125 to 0.125
- w_beta: bfloat16 [2048, 16], P(None, 'tp'), may hold values from -0.125 to 0.125
- w_decay: bfloat16 [2048, 16], P(None, 'tp'), may hold values from -0.125 to 0.125
- decay_rate: float32 [16], P('tp'), may hold values from 0.5 to 8
- decay_bias: float32 [16], P('tp'), may hold values from -3 to 0
- head_gain: float32 [128], replicated, may hold values from 0.1 to 1.9
- state: float32 [256, 16, 128, 128], P('ep', 'tp'), may hold values from -1.5 to 1.5
- w_out: bfloat16 [2048, 2048], P('tp', 'ep'), may hold values from -0.125 to 0.125
- moe_gain: float32 [2048], replicated, may hold values from 0.1 to 1.9
- dense_mix: bfloat16 [2048], replicated, may hold values from -0.125 to 0.125
- dense_gate: bfloat16 [2048, 4096], P(None, ('ep', 'tp')), may hold values from -0.125 to 0.125
- dense_up: bfloat16 [2048, 4096], P(None, ('ep', 'tp')), may hold values from -0.125 to 0.125
- dense_down: bfloat16 [4096, 2048], P(('ep', 'tp')), may hold values from -0.09375 to 0.09375
- expert_gate: bfloat16 [16, 2048, 1024], P('ep', None, 'tp'), may hold values from -0.125 to 0.125
- expert_up: bfloat16 [16, 2048, 1024], P('ep', None, 'tp'), may hold values from -0.125 to 0.125
- expert_down: bfloat16 [16, 1024, 2048], P('ep', 'tp'), may hold values from -0.1875 to 0.1875
- expert_ids: int32 [256, 4], replicated, may hold values from 0 to 15, as said below
- route_weight: float32 [256, 4], replicated, may hold values from 0.1 to 1
Outputs:
- layer_out: bfloat16 [256, 2048], P(('ep', 'tp'))
- new_state: float32 [256, 16, 128, 128], P('ep', 'tp')
The draws below stay inside these ranges and needn't reach their ends.
Inputs may be any that keep to these rules, and one draw needn't show every extreme that they name: `expert_ids`: the 4 experts of a row are distinct and lie in one group of 8 consecutive ids. In each aligned block of 16 rows (the rows of one index of ep) no expert is named by more than 8 rows, and at most 16 rows pick one group.
All inputs are finite; a program needn't handle non-finite values.
Results may differ from the reference program's by a relative error of at most 0.012.
Values may be sent and summed in bfloat16 or wider, within the bound.
A program may use at most 128 MiB of HBM per device.

```python
import math
import jax
import jax.numpy as jnp
from jax import lax

D = 2048
HEADS = 16
HEAD = 128
FFE = 1024
FFD = 4096
EPG = 8
TOP_K = 4
SEQ_GROUP = 16
HD = 2048
EXPERTS = 16
GROUPS = 2
GCAP = 16
CAP = 8
SLOTS = 128
TOKENS = 256


def draw_expert_ids(key, part):
    base = jax.random.fold_in(key, 11)
    key_hot, key_blocks = jax.random.split(base)
    hot_base = jax.random.randint(key_hot, (), 0, GROUPS)
    block_count = TOKENS // SEQ_GROUP

    def one_block(block_key, block_number):
        hot_group = (hot_base + block_number) % GROUPS
        key_pool, key_order, key_labels = jax.random.split(block_key, 3)
        others = (hot_group + 1 + jnp.repeat(jnp.arange(GROUPS - 1, dtype=jnp.int32), GCAP)) % GROUPS
        others = jax.random.permutation(key_pool, others)
        pool = jnp.concatenate([jnp.full((GCAP,), hot_group, jnp.int32), others.astype(jnp.int32)])[:SEQ_GROUP]
        groups = jax.random.permutation(key_order, pool)
        positions = jnp.arange(SEQ_GROUP, dtype=jnp.int32)
        same_group = groups[:, None] == groups[None, :]
        earlier = positions[None, :] < positions[:, None]
        rank_in = jnp.sum((same_group & earlier).astype(jnp.int32), axis=1)
        local = (rank_in[:, None] * TOP_K + jnp.arange(TOP_K, dtype=jnp.int32)[None, :]) % EPG
        labels = jax.vmap(lambda label_key: jax.random.permutation(label_key, EPG))(jax.random.split(key_labels, GROUPS)).astype(jnp.int32)
        chosen = labels[groups[:, None], local]
        return (groups[:, None] * EPG + chosen).astype(jnp.int32)
    blocks = jax.vmap(one_block)(jax.random.split(key_blocks, block_count), jnp.arange(block_count, dtype=jnp.int32))
    return blocks.reshape(TOKENS, TOP_K).astype(jnp.int32)


def shard_levels(key, dims, pieces, smallest, largest):
    level = 1.0
    for position, blocks in pieces:
        draws = jax.random.uniform(jax.random.fold_in(jax.random.fold_in(key, 6), position), (blocks,), jnp.float32, smallest / len(pieces), largest / len(pieces))
        level = level * jnp.repeat(jnp.exp(draws), dims[position] // blocks).reshape((-1,) + (1,) * (len(dims) - 1 - position))
    return level


def bell_draw(key, shape, scale, most, cuts=(), kind=jnp.bfloat16):
    drawn = scale * jax.random.normal(key, shape, jnp.float32)
    if cuts:
        drawn = drawn * shard_levels(key, shape, cuts, -0.22, 0.18)
    return jnp.clip(drawn, -most, most).astype(kind)


def setup_inputs(seed: int = 0) -> dict:
    streams_of = jax.random.split(jax.random.key(seed), 24)
    return {
        "tokens": bell_draw(streams_of[0], (TOKENS, D), 1.0, 6.0, ((0, 32),)),
        "mix_gain": jnp.clip(1.0 + 0.18 * jax.random.normal(streams_of[1], (D,), jnp.float32), 0.1, 1.9),
        "w_query": bell_draw(streams_of[2], (D, HEADS, HEAD), D ** -0.5, 0.125, ((1, 2), (2, 16))),
        "w_key": bell_draw(streams_of[3], (D, HEADS, HEAD), D ** -0.5, 0.125, ((1, 2), (2, 16))),
        "w_value": bell_draw(streams_of[4], (D, HEADS, HEAD), D ** -0.5, 0.125, ((1, 2), (2, 16))),
        "w_zgate": bell_draw(streams_of[5], (D, HEADS, HEAD), D ** -0.5, 0.125, ((1, 2), (2, 16))),
        "w_beta": bell_draw(streams_of[6], (D, HEADS), D ** -0.5, 0.125, ((1, 2),)),
        "w_decay": bell_draw(streams_of[7], (D, HEADS), D ** -0.5, 0.125, ((1, 2),)),
        "decay_rate": jnp.clip(jnp.exp(math.log(8.0) - 2.7725887 * jax.random.uniform(streams_of[8], (HEADS,), jnp.float32) ** shard_levels(streams_of[8], (HEADS,), ((0, 2),), -0.2, 0.2)), 0.5, 8.0),
        "decay_bias": jnp.clip(-3.0 + 3.0 * jax.random.uniform(streams_of[9], (HEADS,), jnp.float32) ** shard_levels(streams_of[9], (HEADS,), ((0, 2),), -0.2, 0.2), -3.0, 0.0),
        "head_gain": jnp.clip(1.0 + 0.18 * jax.random.normal(streams_of[10], (HEAD,), jnp.float32), 0.1, 1.9),
        "state": bell_draw(streams_of[11], (TOKENS, HEADS, HEAD, HEAD), 0.25, 1.5, ((0, 16), (1, 2)), jnp.float32),
        "w_out": bell_draw(streams_of[12], (HD, D), HD ** -0.5, 0.125, ((0, 2), (1, 16))),
        "moe_gain": jnp.clip(1.0 + 0.18 * jax.random.normal(streams_of[13], (D,), jnp.float32), 0.1, 1.9),
        "dense_mix": bell_draw(streams_of[14], (D,), D ** -0.5, 0.125),
        "dense_gate": bell_draw(streams_of[15], (D, FFD), D ** -0.5, 0.125, ((1, 32),)),
        "dense_up": bell_draw(streams_of[16], (D, FFD), D ** -0.5, 0.125, ((1, 32),)),
        "dense_down": bell_draw(streams_of[17], (FFD, D), FFD ** -0.5, 0.09375, ((0, 32),)),
        "expert_gate": bell_draw(streams_of[18], (EXPERTS, D, FFE), D ** -0.5, 0.125, ((0, 16), (2, 2))),
        "expert_up": bell_draw(streams_of[19], (EXPERTS, D, FFE), D ** -0.5, 0.125, ((0, 16), (2, 2))),
        "expert_down": bell_draw(streams_of[20], (EXPERTS, FFE, D), FFE ** -0.5, 0.1875, ((0, 16), (1, 2))),
        "expert_ids": draw_expert_ids(jax.random.fold_in(streams_of[23], 71), 0),
        "route_weight": jnp.clip(jnp.exp(jax.random.uniform(streams_of[22], (TOKENS, TOP_K), jnp.float32, math.log(0.1), math.log(1.0))), 0.1, 1.0),
    }


EPS = 1e-06

def rms_scale(values, gain):
    return values * lax.rsqrt(lax.optimization_barrier(jnp.mean(values * values, axis=-1, keepdims=True)) + EPS) * gain

def unit_rows(values):
    return values * lax.rsqrt(lax.optimization_barrier(jnp.sum(values * values, axis=-1, keepdims=True)) + EPS)

def reference(tokens, mix_gain, w_query, w_key, w_value, w_zgate, w_beta, w_decay, decay_rate, decay_bias, head_gain, state, w_out, moe_gain, dense_mix, dense_gate, dense_up, dense_down, expert_gate, expert_up, expert_down, expert_ids, route_weight):
    tok_float = tokens.astype(jnp.float32)
    normed = rms_scale(tok_float, mix_gain).astype(jnp.bfloat16)

    def project(weight):
        product = jnp.dot(normed, weight.reshape(D, HD), preferred_element_type=jnp.float32)
        return product.astype(jnp.bfloat16).reshape(TOKENS, HEADS, HEAD).astype(jnp.float32)
    query = unit_rows(jax.nn.silu(project(w_query))) * HEAD ** (-0.5)
    key_vec = unit_rows(jax.nn.silu(project(w_key)))
    value = jax.nn.silu(project(w_value))
    gate_in = project(w_zgate)
    beta_rate = jax.nn.sigmoid(jnp.dot(normed, w_beta, preferred_element_type=jnp.float32))
    decay_in = jnp.dot(normed, w_decay, preferred_element_type=jnp.float32)
    retain = jnp.exp(-decay_rate * jax.nn.softplus(decay_in + decay_bias))
    recalled = jnp.einsum('shkv,shk->shv', state, key_vec, precision=lax.Precision.HIGHEST)
    correction = value - retain[..., None] * recalled
    new_state = retain[..., None, None] * state + (beta_rate[..., None] * key_vec)[..., :, None] * correction[..., None, :]
    readout = jnp.einsum('shkv,shk->shv', new_state, query, precision=lax.Precision.HIGHEST)
    gated = rms_scale(readout, head_gain) * jax.nn.silu(gate_in)
    gated = gated.astype(jnp.bfloat16).reshape(TOKENS, HD)
    resid = tok_float + jnp.dot(gated, w_out, preferred_element_type=jnp.float32)
    moe_in = rms_scale(resid, moe_gain).astype(jnp.bfloat16)
    dense_hidden = (jax.nn.silu(jnp.dot(moe_in, dense_gate, preferred_element_type=jnp.float32)) * jnp.dot(moe_in, dense_up, preferred_element_type=jnp.float32)).astype(jnp.bfloat16)
    mix_factor = jax.nn.sigmoid(jnp.dot(moe_in, dense_mix, preferred_element_type=jnp.float32))
    dense_out = mix_factor[:, None] * jnp.dot(dense_hidden, dense_down, preferred_element_type=jnp.float32)
    positions = jnp.arange(TOKENS, dtype=jnp.int32)
    block_idx = positions // SEQ_GROUP
    slot_iota = jnp.arange(SLOTS, dtype=jnp.int32)

    def one_expert(summed, stacked):
        expert, gate_w, up_w, down_w = stacked
        matched = expert_ids == expert
        routed = jnp.any(matched, axis=1).astype(jnp.int32)
        weight = lax.optimization_barrier(jnp.sum(jnp.where(matched, route_weight, 0.0), axis=1))
        rank_in = (jnp.cumsum(routed.reshape(-1, SEQ_GROUP), axis=1).reshape(-1) - routed).astype(jnp.int32)
        slot_idx = (block_idx * CAP + rank_in).astype(jnp.int32)
        matches = (slot_idx[None, :] == slot_iota[:, None]) & (routed[None, :] > 0)
        source = lax.optimization_barrier(jnp.sum(jnp.where(matches, positions[None, :], 0), axis=1)).astype(jnp.int32)
        picked = jnp.take(moe_in, source, axis=0)
        expert_hidden = (jax.nn.silu(jnp.dot(picked, gate_w, preferred_element_type=jnp.float32)) * jnp.dot(picked, up_w, preferred_element_type=jnp.float32)).astype(jnp.bfloat16)
        expert_out = jnp.dot(expert_hidden, down_w, preferred_element_type=jnp.float32)
        row_take = jnp.take(expert_out, jnp.minimum(slot_idx, SLOTS - 1), axis=0)
        return (summed + weight[:, None] * row_take, None)
    moe_out, _ = lax.scan(one_expert, jnp.zeros((TOKENS, D), jnp.float32), (jnp.arange(EXPERTS, dtype=jnp.int32), expert_gate, expert_up, expert_down))
    layer_out = (resid + dense_out + moe_out).astype(jnp.bfloat16)
    return (layer_out, new_state)
```

```python
import functools

import jax
import jax.numpy as jnp
from jax import lax
from jax.experimental import pallas as pl
from jax.experimental.pallas import tpu as pltpu
from jax.sharding import PartitionSpec as P

EPS = 1e-06
VMEM = pltpu.VMEM
ANY = pl.ANY
MESH = pl.DeviceIdType.MESH
NARROW, FULL = jnp.bfloat16, jnp.float32


def rms_scale(values, gain):
    return values * lax.rsqrt(jnp.mean(values * values, axis=-1, keepdims=True) + EPS) * gain


def silu(v):
    return v / (1.0 + jnp.exp(-v))


def grid_of(count):
    for depth in (4, 2, 1):
        side = int(round((count / depth) ** 0.5))
        if depth * side * side == count:
            return depth, side
    return count, 1


def place_of(count, ep, t):
    depth, side = grid_of(count)
    z = ep // (side * side)
    y = (ep // side) % side
    x = ep % side
    a = x * (1 - t) + y * t
    b = y * (1 - t) + x * t
    return z, b, a


def place(count):
    depth, side = grid_of(count)
    t = lax.axis_index("tp")
    z, b, a = place_of(count, lax.axis_index("ep"), t)
    return depth, side, t, z, b, a


def ep_of(side, t, z, b, a):
    y = b * (1 - t) + a * t
    x = a * (1 - t) + b * t
    return (z * side + y) * side + x


def slot_of(depth, side, z, b, a):
    return (a * side + b) * depth + z


def flip(v, i):
    out = v
    bit = 1
    while bit <= i:
        if i & bit:
            out = out + bit - 2 * bit * ((v // bit) % 2)
        bit *= 2
    return out


def other_core():
    return (lax.axis_index("ep"), 1 - lax.axis_index("tp"))


def near(count):
    depth, side, t, z, b, a = place(count)
    steps = [(flip(z, i), b, a) for i in range(1, depth)]
    steps += [(z, flip(b, i), a) for i in range(1, side)]
    steps += [(z, b, flip(a, i)) for i in range(1, side)]
    return [(ep_of(side, t, *c), t) for c in steps]


def greet(devices):
    barrier = pltpu.get_barrier_semaphore()
    for device in devices:
        pl.semaphore_signal(barrier, inc=1, device_id=device, device_id_type=MESH)
    return len(devices)


def greet_all(count):
    barrier = pltpu.get_barrier_semaphore()
    me = lax.axis_index("ep") * 2 + lax.axis_index("tp")

    def hello(i, carry):
        other = lax.rem(me + i, 2 * count)
        pl.semaphore_signal(
            barrier, inc=1, device_id=(other // 2, other % 2), device_id_type=MESH
        )
        return carry

    lax.fori_loop(1, count * 2, hello, 0)
    return 2 * count - 1


def remote(src, dst, send_sem, recv_sem, device):
    return pltpu.make_async_remote_copy(
        src_ref=src,
        dst_ref=dst,
        send_sem=send_sem,
        recv_sem=recv_sem,
        device_id=device,
        device_id_type=MESH,
    )


def gather(count, pieces, send_sem, recv_sem):
    depth, side, t, z, b, a = place(count)
    number = [0]
    started = []
    arrivals = {}
    peers = {
        "z": [(i, 0, 0) for i in range(1, depth)],
        "b": [(0, i, 0) for i in range(1, side)],
        "a": [(0, 0, i) for i in range(1, side)],
    }
    nothing = (0, 0, 0)
    plus = lambda u, v: tuple(i ^ j for i, j in zip(u, v))

    def at(offset):
        dz, db, da = offset
        return flip(z, dz), flip(b, db), flip(a, da)

    def relay(p, offset, legs):
        source, view, _, _ = pieces[p]
        spot = view(*at(offset))
        for leg in legs:
            for step in peers[leg]:
                n = number[0]
                number[0] += 1
                copy = remote(
                    source if offset == nothing and source is not None else spot,
                    spot,
                    send_sem.at[n],
                    recv_sem.at[n],
                    (ep_of(side, t, *at(step)), t),
                )
                copy.start()
                started.append(copy)
                arrivals[p, leg, plus(offset, step)] = copy

    for p, (_, _, order, arrival) in enumerate(pieces):
        if arrival is not None:
            arrival()
        relay(p, nothing, order)
    for i in range(max(depth, side) - 1):
        for p, (_, _, order, _) in enumerate(pieces):
            if i < len(peers[order[0]]):
                offset = peers[order[0]][i]
                arrivals[p, order[0], offset].wait_recv()
                relay(p, offset, order[1:])
    for p, (_, _, order, _) in enumerate(pieces):
        for first in [nothing] + peers[order[0]]:
            for second in peers[order[1]]:
                offset = plus(first, second)
                arrivals[p, order[1], offset].wait_recv()
                relay(p, offset, order[2:])
    for p, (_, _, order, _) in enumerate(pieces):
        for first in [nothing] + peers[order[0]]:
            for second in [nothing] + peers[order[1]]:
                for third in peers[order[2]]:
                    arrivals[p, order[2], plus(plus(first, second), third)].wait_recv()

    def finish():
        for copy in started:
            copy.wait_send()

    return finish


def contract(left, right):
    return lax.dot_general(left, right, (((1,), (1,)), ((), ())), preferred_element_type=FULL)


def flat_rows(ref):
    blocks, rows, width = ref.shape
    return ref[...].astype(FULL).reshape(blocks * rows, width)


def project_kernel(
    count,
    tokens_ref,
    gain_ref,
    wq_ref,
    wk_ref,
    wv_ref,
    wz_ref,
    beta_ref,
    decay_ref,
    rate_ref,
    bias_ref,
    out_ref,
    columns_ref,
    rows,
    pair,
    normed,
    weights,
    blocks,
    landed,
    flat,
    turned,
    load_sem,
    core_send,
    core_recv,
    send_sem,
    recv_sem,
    send_sem2,
    recv_sem2,
):
    ep = lax.axis_index("ep")
    depth, side, t, z, b, a = place(count)
    partner = other_core()
    per = wq_ref.shape[0]
    heads = beta_ref.shape[0]
    own_rows, width = tokens_ref.shape
    seqs = 2 * own_rows
    total = count * own_rows
    wide = 4 * per
    part = per // heads
    loads = []
    for p, w_ref in enumerate((wq_ref, wk_ref, wv_ref, wz_ref)):
        copy = pltpu.make_async_copy(
            w_ref, weights.at[t, pl.ds(p * per, per)], load_sem.at[p]
        )
        copy.start()
        loads.append(copy)
    expected = greet_all(count)
    my_slot = slot_of(depth, side, z, b, a)
    rows[my_slot] = tokens_ref[...]
    pair[t] = tokens_ref[...]
    source = lax.broadcasted_iota(jnp.int32, (wide, wide), 0)
    target = lax.broadcasted_iota(jnp.int32, (wide, wide), 1)
    inner = source % per
    spot = inner % part * (4 * heads) + source // per * heads + inner // part
    order = jnp.where(target == spot, 1.0, 0.0).astype(NARROW)
    pl.semaphore_wait(pltpu.get_barrier_semaphore(), expected)
    crossed = [remote(tokens_ref, pair.at[t], core_send.at[4], core_recv.at[4], partner)]
    for p, w_ref in enumerate((wq_ref, wk_ref, wv_ref, wz_ref)):
        crossed.append(
            remote(
                w_ref,
                weights.at[t, pl.ds(p * per, per)],
                core_send.at[p],
                core_recv.at[p],
                partner,
            )
        )
    for copy in crossed:
        copy.start()
    view = lambda z, b, a: rows.at[slot_of(depth, side, z, b, a)]
    finish = gather(count, [(tokens_ref, view, "zba", None)], send_sem, recv_sem)
    gain = gain_ref[...]
    for i in range(0, count, 2):
        two = jnp.concatenate([rows[i].astype(FULL), rows[i + 1].astype(FULL)], axis=0)
        normed[i * own_rows : (i + 2) * own_rows] = rms_scale(two, gain).astype(NARROW)
    for copy in loads:
        copy.wait()
    for copy in crossed:
        copy.wait_recv()
    left = normed[...]
    for h in range(2):
        product = contract(left, weights[h]).astype(NARROW)
        moved = jnp.dot(product, order, preferred_element_type=FULL)
        blocks[h] = moved.reshape(count, own_rows, wide).astype(NARROW)
    me = ep * 2 + t

    def copy_to(i):
        other = lax.rem(me + i, 2 * count)
        oe, ot = other // 2, other % 2
        oz, ob, oa = place_of(count, oe, t)
        return remote(
            blocks.at[ot, slot_of(depth, side, oz, ob, oa)],
            landed.at[ep, t],
            send_sem2.at[i],
            recv_sem2.at[i],
            (oe, ot),
        )

    def start(i, carry):
        copy_to(i).start()
        return carry

    def end(i, carry):
        copy_to(i).wait()
        return carry

    lax.fori_loop(1, 2 * count, start, 0)
    landed[ep, t] = blocks[t, my_slot]
    cols = columns_ref.shape[1]
    if cols % 128 == 0:
        span = pl.ds(pl.multiple_of(ep * cols, 128), cols)
        picked = rows[:, :, span].astype(FULL).reshape(total, cols)
    else:
        line = lax.broadcasted_iota(jnp.int32, (width, cols), 0)
        lane = lax.broadcasted_iota(jnp.int32, (width, cols), 1)
        one = jnp.where(line == lane + ep * cols, 1.0, 0.0).astype(NARROW)
        picked = jnp.dot(flat_rows(rows).astype(NARROW), one, preferred_element_type=FULL)
    columns_ref[...] = picked
    seq = rms_scale(flat_rows(pair), gain).astype(NARROW)
    line = lax.broadcasted_iota(jnp.int32, (heads, heads), 0)
    lane = lax.broadcasted_iota(jnp.int32, (heads, heads), 1)
    tall = lambda v: jnp.sum(jnp.where(line == lane, v, 0.0), axis=1, keepdims=True)
    beta = 1.0 / (1.0 + jnp.exp(-contract(beta_ref[...], seq)))
    pre = contract(decay_ref[...], seq) + tall(bias_ref[...])
    soft = jnp.maximum(pre, 0.0) + jnp.log1p(jnp.exp(-jnp.abs(pre)))
    retain = jnp.exp(-tall(rate_ref[...]) * soft)
    size = out_ref.shape[2]
    for s in range(seqs):
        out_ref[s, 4 * heads : 5 * heads, :] = jnp.broadcast_to(beta[:, s : s + 1], (heads, size))
        out_ref[s, 5 * heads :, :] = jnp.broadcast_to(retain[:, s : s + 1], (heads, size))
    finish()
    for copy in crossed:
        copy.wait_send()
    lax.fori_loop(1, 2 * count, end, 0)
    lanes = 4 * heads
    bunch = 128 // lanes
    arrived = landed[...].astype(FULL).reshape(count * seqs, wide)
    for q in range(flat.shape[0]):
        span = arrived[:, q * 128 : (q + 1) * 128]
        flat[q, :, : span.shape[1]] = span
    for g in range(seqs // bunch):
        each = [
            [flat[q, pl.ds(g * bunch + s, count, stride=seqs), :] for q in range(flat.shape[0])]
            for s in range(bunch)
        ]
        for j in range(part):
            q, i = j // bunch, j % bunch
            piece = [v[q][:, i * lanes : (i + 1) * lanes] for v in each]
            piece = jnp.concatenate(piece, axis=1)
            turned[pl.ds(j, count, stride=part), :] = piece
        lines = silu(jnp.transpose(turned[...])).reshape(bunch, 4, heads, size)
        for s in range(bunch):
            for p in range(4):
                v = lines[s, p]
                if p < 2:
                    v = v * lax.rsqrt(jnp.sum(v * v, axis=-1, keepdims=True) + EPS)
                if p == 0:
                    v = v * size ** (-0.5)
                out_ref[g * bunch + s, p * heads : (p + 1) * heads, :] = v


def sems(n):
    return [pltpu.SemaphoreType.DMA((n,)), pltpu.SemaphoreType.DMA((n,))]


def comm_call(kernel, number, out_shape, operands, scratch):
    spec = pl.BlockSpec(memory_space=VMEM)
    return pl.pallas_call(
        kernel,
        out_shape=out_shape,
        in_specs=[pl.BlockSpec(memory_space=ANY) if away else spec for _, away in operands],
        out_specs=jax.tree.map(lambda _: spec, out_shape),
        scratch_shapes=scratch,
        compiler_params=pltpu.CompilerParams(
            collective_id=number, has_side_effects=True, vmem_limit_bytes=60 * 1024 * 1024
        ),
        name=f"stage_{number}",
    )(*[v for v, _ in operands])


def expert_kernel(
    count,
    gated_ref,
    columns_ref,
    gains_ref,
    mix_ref,
    ids_ref,
    route_ref,
    w_ref,
    dg_ref,
    du_ref,
    dd_ref,
    eg_ref,
    eu_ref,
    ed_ref,
    out_ref,
    rows,
    wo,
    dg,
    du,
    dd,
    eg,
    eu,
    ed,
    own,
    every,
    part,
    a_buf,
    sum1,
    b_buf,
    sum2,
    z_buf,
    load_sem,
    core_send,
    core_recv,
    send_sem,
    recv_sem,
    send_sem2,
    recv_sem2,
    send_sem3,
    recv_sem3,
):
    ep = lax.axis_index("ep")
    depth, side, t, z, b, a = place(count)
    partner = other_core()
    own_rows = gated_ref.shape[1]
    half = gated_ref.shape[2]
    total = count * own_rows
    cols = columns_ref.shape[1]
    shards = (w_ref, dg_ref, du_ref, eg_ref, eu_ref, dd_ref, ed_ref)
    places = (wo, dg, du, eg, eu, dd, ed)
    loads = []
    for i, (src, dst) in enumerate(zip(shards, places)):
        copy = pltpu.make_async_copy(src, dst.at[t], load_sem.at[i])
        copy.start()
        loads.append(copy)
    expected = greet([partner] + near(count))
    my_slot = slot_of(depth, side, z, b, a)
    mine = pl.ds(pl.multiple_of(t * half, half), half)
    others = pl.ds(pl.multiple_of((1 - t) * half, half), half)
    rows[my_slot, :, mine] = gated_ref[t]
    weight = jnp.sum(jnp.where(ids_ref[...] == ep, route_ref[...], 0.0), axis=0, keepdims=True)
    tokens = weight.shape[1]
    line = lax.broadcasted_iota(jnp.int32, (total, tokens), 0)
    lane = lax.broadcasted_iota(jnp.int32, (total, tokens), 1)
    place_id = line // own_rows
    chip = ep_of(
        side, t, place_id % depth, (place_id // depth) % side, place_id // (depth * side)
    )
    token = chip * (2 * own_rows) + t * own_rows + line % own_rows
    weight = jnp.sum(jnp.where(token == lane, weight, 0.0), axis=1, keepdims=True)
    pl.semaphore_wait(pltpu.get_barrier_semaphore(), expected)
    there = slot_of(depth, side, *place_of(count, ep, 1 - t))
    swap = remote(
        gated_ref.at[1 - t],
        rows.at[there, :, mine],
        core_send.at[7],
        core_recv.at[7],
        partner,
    )
    swap.start()
    crossed = []
    for i, (src, dst) in enumerate(zip(shards, places)):
        crossed.append(remote(src, dst.at[t], core_send.at[i], core_recv.at[i], partner))

    def arrive():
        swap.wait_recv()
        for copy in crossed:
            copy.start()

    view = lambda span: lambda z, b, a: rows.at[slot_of(depth, side, z, b, a), :, span]
    finish1 = gather(
        count,
        [(gated_ref.at[t], view(mine), "zba", None), (None, view(others), "zba", arrive)],
        send_sem,
        recv_sem,
    )
    loads[0].wait()
    crossed[0].wait_recv()
    flat = flat_rows(rows).astype(NARROW)
    product = jnp.dot(flat[:, :half], wo[0], preferred_element_type=FULL)
    product = product + jnp.dot(flat[:, half:], wo[1], preferred_element_type=FULL)
    resid = columns_ref[...] + product
    own[...] = (resid * gains_ref[pl.ds(ep, 1), :]).astype(NARROW)
    every[ep] = own[...]
    finish2 = gather(
        count,
        [(own, lambda z, b, a: every.at[ep_of(side, t, z, b, a)], "zba", None)],
        send_sem2,
        recv_sem2,
    )
    mixes = mix_ref[...].astype(FULL)
    inverse = 1.0 / gains_ref[...]
    squares = jnp.zeros((total, cols), FULL)
    mixed = jnp.zeros((total, cols), FULL)
    for e in range(count):
        v = every[e].astype(FULL)
        r = v * inverse[e : e + 1]
        squares = squares + r * r
        mixed = mixed + v * mixes[e : e + 1]
    width = count * cols
    scale = lax.rsqrt(jnp.sum(squares, axis=1, keepdims=True) * (1.0 / width) + EPS)
    mixed = scale * jnp.sum(mixed, axis=1, keepdims=True)
    mixed = 1.0 / (1.0 + jnp.exp(-mixed))
    left = jnp.concatenate([every[e] for e in range(count)], axis=1)
    for i in (1, 2, 3, 4):
        loads[i].wait()
        crossed[i].wait_recv()

    def hidden(gate, up, factor):
        gate = scale * jnp.dot(left, gate, preferred_element_type=FULL)
        up = scale * jnp.dot(left, up, preferred_element_type=FULL)
        return (silu(gate) * up * factor).astype(NARROW)

    join = lambda ref: jnp.concatenate([ref[0], ref[1]], axis=1)
    acts = [hidden(join(dg), join(du), mixed)]
    acts += [hidden(eg[h], eu[h], weight) for h in range(2)]
    for i in (5, 6):
        loads[i].wait()
        crossed[i].wait_recv()
    chunks, step = part.shape[0], part.shape[-1]
    ffd = dd.shape[1]
    number = [0]
    started = []

    def send(src, dst, device):
        n = number[0]
        number[0] += 1
        copy = remote(src, dst, send_sem3.at[n], recv_sem3.at[n], device)
        copy.start()
        started.append(copy)
        return copy

    device_of = lambda z, b, a: (ep_of(side, t, z, b, a), t)
    wait1, wait2, wait3 = {}, {}, {}

    def down(c):
        span = slice(c * step, (c + 1) * step)
        term = jnp.dot(acts[0][:, :ffd], dd[0, :, span], preferred_element_type=FULL)
        term = term + jnp.dot(acts[0][:, ffd:], dd[1, :, span], preferred_element_type=FULL)
        for h in range(2):
            term = term + jnp.dot(acts[1 + h], ed[h, :, span], preferred_element_type=FULL)
        part[c] = term.reshape(part.shape[1:]).astype(NARROW)
        for i in range(1, side):
            far = flip(a, i)
            wait1[c, i] = send(part.at[c, far], a_buf.at[c, i - 1], device_of(z, b, far))

    def second(c):
        sums = part[c, a].astype(FULL)
        for i in range(1, side):
            wait1[c, i].wait_recv()
            sums = sums + a_buf[c, i - 1].astype(FULL)
        sum1[c] = sums.astype(NARROW)
        for i in range(1, side):
            far = flip(b, i)
            wait2[c, i] = send(sum1.at[c, far], b_buf.at[c, i - 1], device_of(z, far, a))

    def third(c):
        sums = sum1[c, b].astype(FULL)
        for i in range(1, side):
            wait2[c, i].wait_recv()
            sums = sums + b_buf[c, i - 1].astype(FULL)
        sum2[c] = sums.astype(NARROW)
        for i in range(1, depth):
            far = flip(z, i)
            wait3[c, i] = send(sum2.at[c, far], z_buf.at[c, i - 1], device_of(far, b, a))

    for c in range(chunks):
        down(c)
    for c in range(chunks):
        second(c)
    line = lax.broadcasted_iota(jnp.int32, (own_rows, total), 0)
    lane = lax.broadcasted_iota(jnp.int32, (own_rows, total), 1)
    pick = jnp.where(lane == line + my_slot * own_rows, 1.0, 0.0).astype(NARROW)
    back = [
        jnp.dot(pick, every[e], preferred_element_type=FULL) * inverse[e : e + 1]
        for e in range(count)
    ]
    resid = jnp.concatenate(back, axis=1)
    for c in range(chunks):
        third(c)
    for c in range(chunks):
        sums = resid[:, c * step : (c + 1) * step] + sum2[c, z].astype(FULL)
        for i in range(1, depth):
            wait3[c, i].wait_recv()
            sums = sums + z_buf[c, i - 1].astype(FULL)
        out_ref[:, c * step : (c + 1) * step] = sums.astype(out_ref.dtype)
    finish1()
    finish2()
    swap.wait_send()
    for copy in crossed + started:
        copy.wait_send()


def delta_kernel(heads, r_ref, gain_ref, state_ref, gated_ref, new_ref, acc):
    step = pl.program_id(0)
    bunch = state_ref.shape[0]
    size = state_ref.shape[2]
    for s in range(bunch):
        query = r_ref[s, 0:heads]
        key = r_ref[s, heads : 2 * heads]
        value = r_ref[s, 2 * heads : 3 * heads]
        gate = r_ref[s, 3 * heads : 4 * heads]
        beta = r_ref[s, 4 * heads : 5 * heads]
        keep = r_ref[s, 5 * heads : 6 * heads]
        both = r_ref[s, 0 : 2 * heads]
        high = both.astype(NARROW)
        low = (both - high.astype(FULL)).astype(NARROW)
        left = jnp.concatenate([high, low], axis=0)
        line = lax.broadcasted_iota(jnp.int32, (2 * heads, size), 0) % heads
        reads = jnp.zeros((2 * heads, size), FULL)
        for h in range(heads):
            got = jnp.dot(left, state_ref[s, h].astype(NARROW), preferred_element_type=FULL)
            reads = jnp.where(line == h, got[: 2 * heads] + got[2 * heads :], reads)
        recalled = reads[heads:]
        write = beta * (value - keep * recalled)
        readout = keep * reads[:heads] + jnp.sum(key * query, axis=1, keepdims=True) * write
        gated = rms_scale(readout, gain_ref[...]) * gate
        first = pl.multiple_of((step * bunch + s) * heads, heads)
        acc[pl.ds(first, heads), :] = gated
        split = lambda v: (
            v.astype(NARROW).astype(FULL),
            (v - v.astype(NARROW).astype(FULL)),
        )
        k_high, k_low = split(key)
        w_high, w_low = split(write)
        none = jnp.zeros_like(key)
        tall = jnp.transpose(jnp.concatenate([k_high, k_high, k_low, none], axis=0)).astype(NARROW)
        across = jnp.concatenate([w_high, w_low, w_high, none], axis=0)
        row = lax.broadcasted_iota(jnp.int32, across.shape, 0) % heads
        for h in range(0, heads, 2):
            two = jnp.concatenate(
                [jnp.where(row == h + i, across, 0.0) for i in range(2)], axis=1
            ).astype(NARROW)
            outer = jnp.dot(tall, two, preferred_element_type=FULL)
            for i in range(2):
                new_ref[s, h + i] = (
                    keep[h + i : h + i + 1] * state_ref[s, h + i]
                    + outer[:, i * size : (i + 1) * size]
                )

    @pl.when(step == pl.num_programs(0) - 1)
    def _():
        halves, rows = gated_ref.shape[:2]
        for i in range(halves):
            for h in range(heads):
                piece = acc[pl.ds(i * rows * heads + h, rows, stride=heads), :]
                gated_ref[i, :, h * size : (h + 1) * size] = piece.astype(gated_ref.dtype)


def delta(ready, gain, state):
    seqs, heads, size, _ = state.shape
    bunch = 2
    own = lambda *shape: pl.BlockSpec((bunch,) + shape, lambda s: (s,) + (0,) * len(shape))
    return pl.pallas_call(
        functools.partial(delta_kernel, heads),
        grid=(seqs // bunch,),
        out_shape=(
            jax.ShapeDtypeStruct((2, seqs // 2, heads * size), NARROW),
            jax.ShapeDtypeStruct(state.shape, state.dtype),
        ),
        in_specs=[
            own(*ready.shape[1:]),
            pl.BlockSpec((1, size), lambda s: (0, 0)),
            own(heads, size, size),
        ],
        out_specs=(
            pl.BlockSpec((2, seqs // 2, heads * size), lambda s: (0, 0, 0)),
            own(heads, size, size),
        ),
        scratch_shapes=[VMEM((seqs * heads, size), FULL)],
        compiler_params=pltpu.CompilerParams(dimension_semantics=("arbitrary",)),
        name="delta",
    )(ready, gain.reshape(1, size), state)


def body(
    tokens,
    mix_gain,
    w_query,
    w_key,
    w_value,
    w_zgate,
    w_beta,
    w_decay,
    decay_rate,
    decay_bias,
    head_gain,
    state,
    w_out,
    moe_gain,
    dense_mix,
    dense_gate,
    dense_up,
    dense_down,
    expert_gate,
    expert_up,
    expert_down,
    expert_ids,
    route_weight,
):
    count = lax.axis_size("ep")
    own_rows, width = tokens.shape
    seqs, heads, size, _ = state.shape
    depth, side = grid_of(count)
    total = count * own_rows
    turned = [
        w.transpose(1, 2, 0).reshape(-1, width) for w in (w_query, w_key, w_value, w_zgate)
    ]
    wide = 4 * turned[0].shape[0]
    cols = w_out.shape[1]
    ready, columns = comm_call(
        functools.partial(project_kernel, count),
        1,
        (
            jax.ShapeDtypeStruct((seqs, 6 * heads, size), FULL),
            jax.ShapeDtypeStruct((total, cols), FULL),
        ),
        [(tokens, False), (mix_gain.reshape(1, width), False)]
        + [(w, True) for w in turned]
        + [(w_beta.T, False), (w_decay.T, False)]
        + [(decay_rate.reshape(1, heads), False), (decay_bias.reshape(1, heads), False)],
        [
            VMEM((count, own_rows, width), NARROW),
            VMEM((2, own_rows, width), NARROW),
            VMEM((total, width), NARROW),
            VMEM((2, wide, width), NARROW),
            VMEM((2, count, own_rows, wide), NARROW),
            VMEM((count, 2, own_rows, wide), NARROW),
            VMEM((-(-wide // 128), count * seqs, 128), FULL),
            VMEM((size, 128), FULL),
            pltpu.SemaphoreType.DMA((4,)),
        ]
        + sems(5)
        + sems(count - 1)
        + sems(2 * count),
    )
    gated, new_state = delta(ready, head_gain, state)
    chunks = 4
    step = width // chunks
    shard = lambda w: VMEM((2,) + w.shape, NARROW)
    held = (w_out, dense_gate, dense_up, dense_down, expert_gate[0], expert_up[0], expert_down[0])
    layer_out = comm_call(
        functools.partial(expert_kernel, count),
        2,
        jax.ShapeDtypeStruct((own_rows, width), NARROW),
        [
            (gated, False),
            (columns, False),
            (moe_gain.reshape(count, cols), False),
            (dense_mix.reshape(count, cols), False),
            (expert_ids.T, False),
            (route_weight.T, False),
        ]
        + [(w, True) for w in held],
        [VMEM((count, own_rows, width), NARROW)]
        + [shard(w) for w in held]
        + [
            VMEM((total, cols), NARROW),
            VMEM((count, total, cols), NARROW),
            VMEM((chunks, side, side, depth, own_rows, step), NARROW),
            VMEM((chunks, max(side - 1, 1), side, depth, own_rows, step), NARROW),
            VMEM((chunks, side, depth, own_rows, step), NARROW),
            VMEM((chunks, max(side - 1, 1), depth, own_rows, step), NARROW),
            VMEM((chunks, depth, own_rows, step), NARROW),
            VMEM((chunks, max(depth - 1, 1), own_rows, step), NARROW),
            pltpu.SemaphoreType.DMA((7,)),
        ]
        + sems(8)
        + sems(2 * (count - 1))
        + sems(count - 1)
        + sems(chunks * (2 * (side - 1) + depth - 1)),
    )
    return (layer_out, new_state)


def solution(mesh):
    placed = (
        P(("ep", "tp"), None),
        P(),
        P(None, "tp", "ep"),
        P(None, "tp", "ep"),
        P(None, "tp", "ep"),
        P(None, "tp", "ep"),
        P(None, "tp"),
        P(None, "tp"),
        P("tp"),
        P("tp"),
        P(),
        P("ep", "tp", None, None),
        P("tp", "ep"),
        P(),
        P(),
        P(None, ("ep", "tp")),
        P(None, ("ep", "tp")),
        P(("ep", "tp"), None),
        P("ep", None, "tp"),
        P("ep", None, "tp"),
        P("ep", "tp", None),
        P(),
        P(),
    )
    return jax.shard_map(
        body,
        mesh=mesh,
        in_specs=placed,
        out_specs=(P(("ep", "tp"), None), P("ep", "tp", None, None)),
        check_vma=False,
    )
```

```python
import functools
import types

import jax
import jax.numpy as jnp
from jax import lax
from jax.experimental import pallas as pl
from jax.experimental.pallas import tpu as pltpu
from jax.sharding import PartitionSpec as P

EPS = 1e-06
VMEM = pltpu.VMEM
HBM = pltpu.HBM
MESH = pl.DeviceIdType.MESH
NARROW, FULL = jnp.bfloat16, jnp.float32


def rms_scale(values, gain):
    return values * lax.rsqrt(jnp.mean(values * values, axis=-1, keepdims=True) + EPS) * gain


def silu(v):
    return v / (1.0 + jnp.exp(-v))


def grid_of(count):
    for depth in (4, 2, 1):
        side = int(round((count / depth) ** 0.5))
        if depth * side * side == count:
            return depth, side
    return count, 1


def place_of(count, ep, t):
    depth, side = grid_of(count)
    z = ep // (side * side)
    y = (ep // side) % side
    x = ep % side
    a = x * (1 - t) + y * t
    b = y * (1 - t) + x * t
    return z, b, a


def place(count):
    depth, side = grid_of(count)
    t = lax.axis_index("tp")
    z, b, a = place_of(count, lax.axis_index("ep"), t)
    return depth, side, t, z, b, a


def ep_of(side, t, z, b, a):
    y = b * (1 - t) + a * t
    x = a * (1 - t) + b * t
    return (z * side + y) * side + x


def slot_of(depth, side, z, b, a):
    return (z * side + a) * side + b


def flip(v, i):
    out = v
    bit = 1
    while bit <= i:
        if i & bit:
            out = out + bit - 2 * bit * ((v // bit) % 2)
        bit *= 2
    return out


def other_core():
    return (lax.axis_index("ep"), 1 - lax.axis_index("tp"))


def peers_of(count):
    depth, side = grid_of(count)
    plane = [(0, j, i) for j in range(side) for i in range(side)][1:]
    plane.sort(key=lambda o: -(o[1] > 0) - (o[2] > 0))
    return [(i, 0, 0) for i in range(1, depth)], plane


def at(here, offset):
    return tuple(flip(v, i) for v, i in zip(here, offset))


def remote(src, dst, sems, n, device):
    return pltpu.make_async_remote_copy(
        src_ref=src,
        dst_ref=dst,
        send_sem=sems[0].at[n],
        recv_sem=sems[1].at[n],
        device_id=device,
        device_id_type=MESH,
    )


def gather(count, pieces, sems, landed=None, then=None):
    depth, side, t, *here = place(count)
    lines, plane = peers_of(count)
    started = []
    arrivals = {}
    nothing = (0, 0, 0)
    plus = lambda u, v: tuple(i ^ j for i, j in zip(u, v))

    def spread(p, offset, steps):
        source, view, _ = pieces[p]
        spot = view(*at(here, offset))
        if offset == nothing and source is not None:
            source_ref = source
        else:
            source_ref = spot
        for step in steps:
            device = (ep_of(side, t, *at(here, step)), t)
            copy = remote(source_ref, spot, sems, len(started), device)
            copy.start()
            started.append(copy)
            arrivals[p, plus(offset, step)] = copy

    for p, (_, _, arrival) in enumerate(pieces):
        if arrival is not None:
            arrival()
        spread(p, nothing, plane + lines)
    if then is not None:
        then()
    for offset in lines:
        for p in range(len(pieces)):
            arrivals[p, offset].wait_recv()
            spread(p, offset, plane)
    for offset in [nothing] + lines:
        for p in range(len(pieces)):
            for step in plane:
                arrivals[p, plus(offset, step)].wait_recv()
        if landed is not None:
            landed(offset[0])

    def finish():
        for copy in started:
            copy.wait_send()

    return finish


def contract(left, right):
    return lax.dot_general(left, right, (((1,), (1,)), ((), ())), preferred_element_type=FULL)


def dot(left, right):
    return jnp.dot(left, right, preferred_element_type=FULL)


def flat_rows(ref):
    blocks, rows, width = ref.shape
    return ref[...].astype(FULL).reshape(blocks * rows, width)


def grid_ids(*shape):
    return tuple(lax.broadcasted_iota(jnp.int32, shape, i) for i in range(2))


def sigmoid(v):
    return 1.0 / (1.0 + jnp.exp(-v))


def layer_kernel(count, names, pairs, *refs):
    r = types.SimpleNamespace(**dict(zip(names, refs)))
    for name in pairs:
        setattr(r, name, (getattr(r, name + "_send"), getattr(r, name + "_recv")))
    ep = lax.axis_index("ep")
    depth, side, t, *here = place(count)
    z, b, a = here
    lines, plane = peers_of(count)
    partner = (ep, 1 - t)
    own_rows, width = r.tokens.shape
    seqs = 2 * own_rows
    total = count * own_rows
    per = r.wq_hbm.shape[0]
    wide = 4 * per
    heads = r.beta.shape[0]
    part = per // heads
    size = width // (2 * heads)
    half = heads * size
    cols = r.wo.shape[2]
    my_slot = slot_of(depth, side, *here)
    slots = lambda ref: lambda z, b, a: ref.at[slot_of(depth, side, z, b, a)]

    loads = {}

    def load(name, src, dst):
        copy = pltpu.make_async_copy(src, dst, r.load_sem.at[len(loads)])
        copy.start()
        loads[name] = copy

    small = ("tokens", "gain", "beta", "decay", "rate", "bias", "head_gain")
    late = ("moe_gain", "mix", "ids", "route")
    for name in small:
        load(name, getattr(r, name + "_hbm"), getattr(r, name))
    projections = (r.wq_hbm, r.wk_hbm, r.wv_hbm, r.wz_hbm)
    spot_of = lambda p: r.weights.at[t, pl.ds(p * per, per)]
    for p, src in enumerate(projections):
        load(("w", p), src, spot_of(p))
    for s in range(seqs):
        load(("state", s), r.state_hbm.at[s], r.state.at[s])
    for name in late:
        load(name, getattr(r, name + "_hbm"), getattr(r, name))
    shards = ("wo", "dg", "du", "eg", "eu", "dd", "ed")
    for name in shards:
        load(name, getattr(r, name + "_hbm"), getattr(r, name).at[t])

    barrier = pltpu.get_barrier_semaphore()
    devices = [partner] + [(ep_of(side, t, *at(here, o)), t) for o in plane + lines]
    for device in devices:
        pl.semaphore_signal(barrier, inc=1, device_id=device, device_id_type=MESH)
    source, target = grid_ids(wide, wide)
    inner = source % per
    spot = inner % part * (4 * heads) + source // per * heads + inner // part
    order = jnp.where(target == spot, 1.0, 0.0).astype(NARROW)
    loads["tokens"].wait()
    r.rows[my_slot] = r.tokens[...]
    r.pair[t] = r.tokens[...]
    pl.semaphore_wait(barrier, len(devices))

    crossed = {}

    def cross(name, src, dst):
        copy = remote(src, dst, r.core, len(crossed), partner)
        copy.start()
        crossed[name] = copy

    def begin():
        cross("pair", r.tokens, r.pair.at[t])
        for p, src in enumerate(projections):
            cross(("w", p), src, spot_of(p))

    loads["gain"].wait()
    gain = r.gain[...]
    square = side * side

    def normalise(i):
        far = flip(z, i)
        for k in range(0, square, 2):
            first = far * square + k
            two = [r.rows[first + j].astype(FULL) for j in range(2)]
            two = rms_scale(jnp.concatenate(two, axis=0), gain).astype(NARROW)
            start = pl.multiple_of(first * own_rows, 2 * own_rows)
            r.normed[pl.ds(start, 2 * own_rows)] = two

    finish1 = gather(
        count, [(r.tokens, slots(r.rows), None)], r.ring1, normalise, then=begin
    )
    for p in range(4):
        loads["w", p].wait()
        crossed["w", p].wait_recv()
    for name in shards:
        cross(name, getattr(r, name + "_hbm"), getattr(r, name).at[t])
    left = r.normed[...]
    for h in range(2):
        product = contract(left, r.weights[h]).astype(NARROW)
        moved = dot(product, order)
        r.blocks[h] = moved.reshape(count, own_rows, wide).astype(NARROW)

    exchange = []
    for offset in [(i, j, k) for i in range(depth) for j in range(side) for k in range(side)][::-1]:
        z2, b2, a2 = at(here, offset)
        other = ep_of(side, t, z2, b2, a2)
        row = slot_of(depth, side, z2, b2, a2)
        for core in (1 - t, t):
            if offset == (0, 0, 0) and core is t:
                continue
            copy = remote(
                r.blocks.at[core, row], r.landed.at[ep, t], r.swap, len(exchange), (other, core)
            )
            copy.start()
            exchange.append(copy)
    r.landed[ep, t] = r.blocks[t, my_slot]

    if cols % 128 == 0:
        span = pl.ds(pl.multiple_of(ep * cols, 128), cols)
        r.columns[...] = r.rows[:, :, span].astype(FULL).reshape(total, cols)
    else:
        line, lane = grid_ids(width, cols)
        one = jnp.where(line == lane + ep * cols, 1.0, 0.0).astype(NARROW)
        r.columns[...] = dot(flat_rows(r.rows).astype(NARROW), one)
    crossed["pair"].wait_recv()
    for name in small[2:]:
        loads[name].wait()
    seq = rms_scale(flat_rows(r.pair), gain).astype(NARROW)
    line, lane = grid_ids(heads, heads)
    tall = lambda v: jnp.sum(jnp.where(line == lane, v, 0.0), axis=1, keepdims=True)
    beta = sigmoid(contract(r.beta[...], seq))
    pre = contract(r.decay[...], seq) + tall(r.bias[...])
    soft = jnp.maximum(pre, 0.0) + jnp.log1p(jnp.exp(-jnp.abs(pre)))
    retain = jnp.exp(-tall(r.rate[...]) * soft)
    for s in range(seqs):
        r.ready[4, s] = jnp.broadcast_to(beta[:, s : s + 1], (heads, size))
        r.ready[5, s] = jnp.broadcast_to(retain[:, s : s + 1], (heads, size))
    for name in late:
        loads[name].wait()
    weight = jnp.sum(jnp.where(r.ids[...] == ep, r.route[...], 0.0), axis=0, keepdims=True)
    line, lane = grid_ids(total, weight.shape[1])
    place_id = line // own_rows
    chip = ep_of(side, t, place_id // square, place_id % side, (place_id // side) % side)
    token = chip * seqs + t * own_rows + line % own_rows
    weight = jnp.sum(jnp.where(token == lane, weight, 0.0), axis=1, keepdims=True)
    r.weight[...] = jnp.broadcast_to(weight, r.weight.shape)
    r.mixes[...] = r.mix[...].astype(FULL)
    finish1()
    for s in range(seqs):
        loads["state", s].wait()
    for copy in exchange:
        copy.wait()

    lanes = 4 * heads
    bunch = 128 // lanes
    arrived = r.landed[...].astype(FULL).reshape(count * seqs, wide)
    planes = r.flat.shape[0]
    for q in range(planes):
        span = arrived[:, q * 128 : (q + 1) * 128]
        r.flat[q, :, : span.shape[1]] = span
    for g in range(seqs // bunch):
        each = [
            [r.flat[q, pl.ds(g * bunch + s, count, stride=seqs), :] for q in range(planes)]
            for s in range(bunch)
        ]
        for j in range(part):
            q, i = j // bunch, j % bunch
            piece = [v[q][:, i * lanes : (i + 1) * lanes] for v in each]
            r.turned[g, pl.ds(j, count, stride=part), :] = jnp.concatenate(piece, axis=1)
    for g in range(seqs // bunch):
        split = silu(jnp.transpose(r.turned[g])).reshape(bunch, 4, heads, size)
        for p in range(4):
            v = split[:, p]
            if p < 2:
                v = v * lax.rsqrt(jnp.sum(v * v, axis=-1, keepdims=True) + EPS)
            if p == 0:
                v = v * size ** (-0.5)
            r.ready[p, g * bunch : (g + 1) * bunch] = v

    there = slot_of(depth, side, *place_of(count, ep, 1 - t))
    mine = pl.ds(pl.multiple_of(t * half, half), half)
    others = pl.ds(pl.multiple_of((1 - t) * half, half), half)
    head_gain = r.head_gain[...]
    line = lax.broadcasted_iota(jnp.int32, (2 * heads, size), 0) % heads

    def readouts(core):
        first = core * own_rows
        reads = []
        for i in range(own_rows):
            s = first + i
            both = jnp.concatenate([r.ready[0, s], r.ready[1, s]], axis=0)
            high = both.astype(NARROW)
            low = (both - high.astype(FULL)).astype(NARROW)
            pushed = jnp.concatenate([high, low], axis=0)
            kept = jnp.zeros((2 * heads, size), FULL)
            for h in range(heads):
                got = dot(pushed, r.state[s, h].astype(NARROW))
                kept = jnp.where(line == h, got[: 2 * heads] + got[2 * heads :], kept)
            reads.append(kept)
        rows = pl.ds(pl.multiple_of(first, own_rows), own_rows)
        query, key, value, gate, beta, keep = (
            r.ready[p, rows].reshape(own_rows * heads, size) for p in range(6)
        )
        recalled = jnp.concatenate([v[heads:] for v in reads], axis=0)
        asked = jnp.concatenate([v[:heads] for v in reads], axis=0)
        write = beta * (value - keep * recalled)
        readout = keep * asked + jnp.sum(key * query, axis=1, keepdims=True) * write
        r.write[rows] = write.reshape(own_rows, heads, size)
        r.acc[...] = rms_scale(readout, head_gain) * gate
        for h in range(heads):
            piece = r.acc[pl.ds(h, own_rows, stride=heads), :]
            r.gated[core, :, h * size : (h + 1) * size] = piece.astype(NARROW)

    readouts(1 - t)
    swap = remote(r.gated.at[1 - t], r.mixed.at[there, :, mine], r.core, len(crossed), partner)
    swap.start()
    readouts(t)
    r.mixed[my_slot, :, mine] = r.gated[t]

    view = lambda span: lambda z, b, a: r.mixed.at[slot_of(depth, side, z, b, a), :, span]

    groups = seqs // bunch

    def prepare():
        keep = r.ready[5].reshape(seqs * heads, size)
        r.pack[2 * groups] = keep.astype(NARROW)
        r.pack[2 * groups + 1] = (keep - keep.astype(NARROW).astype(FULL)).astype(NARROW)
        none = jnp.zeros((heads, size), FULL)
        high = lambda v: v.astype(NARROW).astype(FULL)
        for g in range(groups):
            tall, across = [], []
            for s in range(g * bunch, (g + 1) * bunch):
                key, write = r.ready[1, s], r.write[s]
                tall += [high(key), high(key), key - high(key), none]
                across += [high(write), write - high(write), high(write), none]
            r.pack[g] = jnp.transpose(jnp.concatenate(tall, axis=0)).astype(NARROW)
            r.pack[groups + g] = jnp.concatenate(across, axis=0).astype(NARROW)

    finish2 = gather(
        count,
        [(r.gated.at[t], view(mine), None), (None, view(others), swap.wait_recv)],
        r.ring2,
        then=prepare,
    )
    loads["wo"].wait()
    crossed["wo"].wait_recv()
    flat = flat_rows(r.mixed).astype(NARROW)
    resid = r.columns[...] + dot(flat[:, :half], r.wo[0]) + dot(flat[:, half:], r.wo[1])
    r.own[...] = (resid * r.moe_gain[pl.ds(ep, 1), :]).astype(NARROW)
    r.every[ep] = r.own[...]
    for name in ("dg", "du", "eg", "eu"):
        loads[name].wait()
        crossed[name].wait_recv()

    r.squares[...] = jnp.zeros_like(r.squares)
    r.logits[...] = jnp.zeros_like(r.logits)
    ffe = r.eg.shape[2]
    ffd = r.dg.shape[2]

    def absorb(i):
        far = flip(z, i)
        blocks = [r.every[far * square + k] for k in range(square)]
        squares, logits = r.squares[...], r.logits[...]
        for k, v in enumerate(blocks):
            v = v.astype(FULL)
            u = v / r.moe_gain[pl.ds(far * square + k, 1), :]
            squares = squares + u * u
            logits = logits + v * r.mixes[pl.ds(far * square + k, 1), :]
        r.squares[...], r.logits[...] = squares, logits
        left = jnp.concatenate(blocks, axis=1)
        span = pl.ds(pl.multiple_of(far * (square * cols), square * cols), square * cols)
        for dense, expert, low, high in (
            (r.dg, r.eg, r.dgate, r.egate),
            (r.du, r.eu, r.dup, r.eup),
        ):
            pair = jnp.concatenate([dense[0, span, :], dense[1, span, :]], axis=1)
            terms = [(low, 0, pair), (high, 0, expert[0, span, :]), (high, ffe, expert[1, span, :])]
            for ref, start, right in terms:
                lane = slice(start, start + right.shape[1])
                got = dot(left, right)
                if i:
                    got = got + ref[:, lane]
                ref[:, lane] = got

    finish3 = gather(
        count,
        [(r.own, lambda z, b, a: r.every.at[ep_of(side, t, z, b, a)], None)],
        r.ring3,
        absorb,
    )
    scale = jnp.sum(r.squares[...], axis=1, keepdims=True) * (1.0 / width)
    scale = lax.rsqrt(scale + EPS)
    dense_mix = sigmoid(scale * jnp.sum(r.logits[...], axis=1, keepdims=True))
    weight = r.weight[:, :1]
    for gate, up, act, factor in (
        (r.dgate, r.dup, r.dact, dense_mix),
        (r.egate, r.eup, r.eact, weight),
    ):
        step = min(256, act.shape[1])
        for start in range(0, act.shape[1], step):
            lane = slice(start, start + step)
            value = silu(scale * gate[:, lane]) * (scale * up[:, lane] * factor)
            act[:, lane] = value.astype(NARROW)
    for name in ("dd", "ed"):
        loads[name].wait()
        crossed[name].wait_recv()

    chunks, step = r.part.shape[0], r.part.shape[-1]
    started = []

    def send(src, dst, offset):
        device = (ep_of(side, t, *at(here, offset)), t)
        copy = remote(src, dst, r.reduce, len(started), device)
        copy.start()
        started.append(copy)
        return copy

    first, second = {}, {}
    for c in range(chunks):
        span = slice(c * step, (c + 1) * step)
        term = 0.0
        for h in range(2):
            term = term + dot(r.dact[:, h * ffd : (h + 1) * ffd], r.dd[h, :, span])
            term = term + dot(r.eact[:, h * ffe : (h + 1) * ffe], r.ed[h, :, span])
        r.part[c] = term.reshape(r.part.shape[1:]).astype(NARROW)
        for n, offset in enumerate(plane):
            _, b2, a2 = at(here, offset)
            first[c, n] = send(r.part.at[c, :, a2, b2], r.plane_buf.at[c, n], offset)
    line, lane = grid_ids(own_rows, total)
    pick = jnp.where(lane == line + my_slot * own_rows, 1.0, 0.0).astype(NARROW)
    for e in range(count):
        span = slice(e * cols, (e + 1) * cols)
        r.resid[:, span] = dot(pick, r.every[e]) / r.moe_gain[e : e + 1, :]
    for c in range(chunks):
        sums = r.part[c, :, a, b].astype(FULL)
        for n in range(len(plane)):
            first[c, n].wait_recv()
            sums = sums + r.plane_buf[c, n].astype(FULL)
        r.sums[c] = sums.astype(NARROW)
        for n, offset in enumerate(lines):
            second[c, n] = send(r.sums.at[c, flip(z, offset[0])], r.line_buf.at[c, n], offset)
    for c in range(chunks):
        span = slice(c * step, (c + 1) * step)
        sums = r.resid[:, span] + r.sums[c, z].astype(FULL)
        for n in range(len(lines)):
            second[c, n].wait_recv()
            sums = sums + r.line_buf[c, n].astype(FULL)
        for k in range(0, step, 256):
            two = [sums[:, k + j : k + j + 128] for j in (0, 128)]
            first_row = (c * step + k) // 128 * own_rows
            rows = slice(first_row, first_row + 2 * own_rows)
            r.pack[2 * groups + 2, rows] = jnp.concatenate(two, axis=0).astype(NARROW)
    for finish in (finish2, finish3, swap.wait_send):
        finish()
    for copy in list(crossed.values()) + started:
        copy.wait_send()


def update_kernel(groups, pack_ref, state_ref, new_ref, out_ref, keeps):
    bunch, heads, size = state_ref.shape[:3]
    step = pl.program_id(0)
    per = pl.num_programs(0) // groups

    @pl.when(step == 0)
    def _():
        keeps[...] = pack_ref[2 * groups].astype(FULL) + pack_ref[2 * groups + 1].astype(FULL)
        own_rows, width = out_ref.shape
        for e in range(width // 128):
            rows = pack_ref[2 * groups + 2, e * own_rows : (e + 1) * own_rows]
            out_ref[:, e * 128 : (e + 1) * 128] = rows

    tall = pack_ref[step // per]
    across = pack_ref[groups + step // per].astype(FULL)
    row = lax.broadcasted_iota(jnp.int32, across.shape, 0)
    for s in range(bunch):
        place_in = (step % per) * bunch + s
        first = pl.multiple_of((step * bunch + s) * heads, heads)
        keep = keeps[pl.ds(first, heads)]
        for h in range(0, heads, 2):
            wanted = [place_in * (4 * heads) + h + i for i in range(2)]
            two = [
                jnp.where(
                    (row == w) | (row == w + heads) | (row == w + 2 * heads), across, 0.0
                )
                for w in wanted
            ]
            outer = dot(tall, jnp.concatenate(two, axis=1).astype(NARROW))
            for i in range(2):
                kept = keep[h + i : h + i + 1] * state_ref[s, h + i]
                new_ref[s, h + i] = kept + outer[:, i * size : (i + 1) * size]


def update(groups, pack, state, layer):
    seqs, heads, size, _ = state.shape
    bunch = 2
    own = pl.BlockSpec((bunch, heads, size, size), lambda s: (s, 0, 0, 0))
    return pl.pallas_call(
        functools.partial(update_kernel, groups),
        grid=(seqs // bunch,),
        out_shape=(jax.ShapeDtypeStruct(state.shape, state.dtype), layer),
        in_specs=[pl.BlockSpec(pack.shape, lambda s: (0, 0, 0)), own],
        out_specs=(own, pl.BlockSpec(layer.shape, lambda s: (0, 0))),
        scratch_shapes=[VMEM((seqs * heads, size), FULL)],
        compiler_params=pltpu.CompilerParams(
            dimension_semantics=("arbitrary",), vmem_limit_bytes=12 * 1024 * 1024
        ),
        name="update",
    )(pack, state)


def body(
    tokens,
    mix_gain,
    w_query,
    w_key,
    w_value,
    w_zgate,
    w_beta,
    w_decay,
    decay_rate,
    decay_bias,
    head_gain,
    state,
    w_out,
    moe_gain,
    dense_mix,
    dense_gate,
    dense_up,
    dense_down,
    expert_gate,
    expert_up,
    expert_down,
    expert_ids,
    route_weight,
):
    count = lax.axis_size("ep")
    own_rows, width = tokens.shape
    seqs, heads, size, _ = state.shape
    depth, side = grid_of(count)
    total = count * own_rows
    flatten = lambda w: w.transpose(1, 2, 0).reshape(-1, width)
    cols = w_out.shape[1]
    operands = {
        "tokens": tokens,
        "gain": mix_gain.reshape(1, width),
        "beta": w_beta.T,
        "decay": w_decay.T,
        "rate": decay_rate.reshape(1, heads),
        "bias": decay_bias.reshape(1, heads),
        "head_gain": head_gain.reshape(1, size),
        "moe_gain": moe_gain.reshape(count, cols),
        "mix": dense_mix.reshape(count, cols),
        "ids": expert_ids.T,
        "route": route_weight.T,
    }
    split = {
        "wo": w_out,
        "dg": dense_gate,
        "du": dense_up,
        "dd": dense_down,
        "eg": expert_gate[0],
        "eu": expert_up[0],
        "ed": expert_down[0],
    }
    only = {
        "wq": flatten(w_query),
        "wk": flatten(w_key),
        "wv": flatten(w_value),
        "wz": flatten(w_zgate),
        "state": state,
    }
    wide = 4 * only["wq"].shape[0]
    ffd, ffe = dense_gate.shape[1], expert_gate.shape[2]
    chunks = 4
    room = 55 * 1024 if total * width <= 2**18 else 60 * 1024
    step = width // chunks
    group = 128 // (4 * heads)
    near, flat = side * side - 1, depth - 1
    narrow = lambda *shape: VMEM(shape, NARROW)
    full = lambda *shape: VMEM(shape, FULL)
    scratch = {k: VMEM(v.shape, v.dtype) for k, v in operands.items()}
    scratch |= {k: narrow(2, *v.shape) for k, v in split.items()}
    scratch |= {
        "state": full(*state.shape),
        "rows": narrow(count, own_rows, width),
        "pair": narrow(2, own_rows, width),
        "normed": narrow(total, width),
        "weights": narrow(2, wide, width),
        "blocks": narrow(2, count, own_rows, wide),
        "landed": narrow(count, 2, own_rows, wide),
        "flat": full(-(-wide // 128), count * seqs, 128),
        "turned": full(seqs // group, size, 128),
        "columns": full(total, cols),
        "weight": full(total, 128),
        "mixes": full(count, cols),
        "ready": full(6, seqs, heads, size),
        "write": full(seqs, heads, size),
        "acc": full(own_rows * heads, size),
        "gated": narrow(2, own_rows, heads * size),
        "mixed": narrow(count, own_rows, width),
        "own": narrow(total, cols),
        "every": narrow(count, total, cols),
        "squares": full(total, cols),
        "logits": full(total, cols),
        "dgate": full(total, 2 * ffd),
        "dup": full(total, 2 * ffd),
        "egate": full(total, 2 * ffe),
        "eup": full(total, 2 * ffe),
        "dact": narrow(total, 2 * ffd),
        "eact": narrow(total, 2 * ffe),
        "part": narrow(chunks, depth, side, side, own_rows, step),
        "plane_buf": narrow(chunks, max(near, 1), depth, own_rows, step),
        "sums": narrow(chunks, depth, own_rows, step),
        "line_buf": narrow(chunks, max(flat, 1), own_rows, step),
        "resid": full(own_rows, width),
        "load_sem": pltpu.SemaphoreType.DMA((len(operands) + len(split) + 4 + seqs,)),
    }
    pairs = {
        "core": 1 + 4 + len(split) + 1,
        "ring1": count - 1,
        "ring2": 2 * (count - 1),
        "ring3": count - 1,
        "swap": 2 * count - 1,
        "reduce": chunks * (near + flat),
    }
    for name, n in pairs.items():
        scratch[name + "_send"] = pltpu.SemaphoreType.DMA((n,))
        scratch[name + "_recv"] = pltpu.SemaphoreType.DMA((n,))
    sources = operands | split | only
    outs = {"pack": jax.ShapeDtypeStruct((2 * (seqs // group) + 3, 128, 128), NARROW)}
    names = [k + "_hbm" for k in sources] + list(outs) + list(scratch)
    spec = pl.BlockSpec(memory_space=VMEM)
    pack = pl.pallas_call(
        functools.partial(layer_kernel, count, names, tuple(pairs)),
        out_shape=outs["pack"],
        in_specs=[pl.BlockSpec(memory_space=HBM)] * len(sources),
        out_specs=spec,
        scratch_shapes=list(scratch.values()),
        compiler_params=pltpu.CompilerParams(
            collective_id=1, has_side_effects=True, vmem_limit_bytes=room * 1024
        ),
        cost_estimate=pl.CostEstimate(
            flops=4 * 10**10, bytes_accessed=10**8, transcendentals=0
        ),
        name="layer",
    )(*sources.values())
    layer = jax.ShapeDtypeStruct((own_rows, width), NARROW)
    new_state, layer_out = update(seqs // group, pack, state, layer)
    return (layer_out, new_state)


def solution(mesh):
    placed = (
        P(("ep", "tp"), None),
        P(),
        P(None, "tp", "ep"),
        P(None, "tp", "ep"),
        P(None, "tp", "ep"),
        P(None, "tp", "ep"),
        P(None, "tp"),
        P(None, "tp"),
        P("tp"),
        P("tp"),
        P(),
        P("ep", "tp", None, None),
        P("tp", "ep"),
        P(),
        P(),
        P(None, ("ep", "tp")),
        P(None, ("ep", "tp")),
        P(("ep", "tp"), None),
        P("ep", None, "tp"),
        P("ep", None, "tp"),
        P("ep", "tp", None),
        P(),
        P(),
    )
    return jax.shard_map(
        body,
        mesh=mesh,
        in_specs=placed,
        out_specs=(P(("ep", "tp"), None), P("ep", "tp", None, None)),
        check_vma=False,
    )
```

```python
import functools
import types

import jax
import jax.numpy as jnp
from jax import lax
from jax.experimental import pallas as pl
from jax.experimental.pallas import tpu as pltpu
from jax.sharding import PartitionSpec as P

EPS = 1e-06
VMEM = pltpu.VMEM
HBM = pltpu.HBM
MESH = pl.DeviceIdType.MESH
NARROW, FULL = jnp.bfloat16, jnp.float32


def rms_scale(values, gain):
    return values * lax.rsqrt(jnp.mean(values * values, axis=-1, keepdims=True) + EPS) * gain


def silu(v):
    return v / (1.0 + jnp.exp(-v))


def grid_of(count):
    for depth in (4, 2, 1):
        side = int(round((count / depth) ** 0.5))
        if depth * side * side == count:
            return depth, side
    return count, 1


def place_of(count, ep, t):
    depth, side = grid_of(count)
    z = ep // (side * side)
    y = (ep // side) % side
    x = ep % side
    a = x * (1 - t) + y * t
    b = y * (1 - t) + x * t
    return z, b, a


def place(count):
    depth, side = grid_of(count)
    t = lax.axis_index("tp")
    z, b, a = place_of(count, lax.axis_index("ep"), t)
    return depth, side, t, z, b, a


def ep_of(side, t, z, b, a):
    y = b * (1 - t) + a * t
    x = a * (1 - t) + b * t
    return (z * side + y) * side + x


def slot_of(depth, side, z, b, a):
    return (z * side + a) * side + b


def flip(v, i):
    out = v
    bit = 1
    while bit <= i:
        if i & bit:
            out = out + bit - 2 * bit * ((v // bit) % 2)
        bit *= 2
    return out


def other_core():
    return (lax.axis_index("ep"), 1 - lax.axis_index("tp"))


def peers_of(count):
    depth, side = grid_of(count)
    plane = [(0, j, i) for j in range(side) for i in range(side)][1:]
    plane.sort(key=lambda o: -(o[1] > 0) - (o[2] > 0))
    return [(i, 0, 0) for i in range(1, depth)], plane


def at(here, offset):
    return tuple(flip(v, i) for v, i in zip(here, offset))


def remote(src, dst, sems, n, device):
    return pltpu.make_async_remote_copy(
        src_ref=src,
        dst_ref=dst,
        send_sem=sems[0].at[n],
        recv_sem=sems[1].at[n],
        device_id=device,
        device_id_type=MESH,
    )


def gather(count, pieces, sems, whole, landed=None, then=None):
    depth, side, t, *here = place(count)
    lines, plane = peers_of(count)
    nothing = (0, 0, 0)
    send_sem, recv_sem = sems
    arrivals = {}
    grouped = len(pieces) * len(lines)

    def spread(p, offset, steps):
        source, view, _ = pieces[p]
        spot = view(*at(here, offset))
        for step in steps:
            line = step in lines
            n = p * len(lines) + step[0] - 1 if line else grouped + offset[0]
            copy = pltpu.make_async_remote_copy(
                src_ref=source if offset == nothing else spot,
                dst_ref=spot,
                send_sem=send_sem.at[0],
                recv_sem=recv_sem.at[n],
                device_id=(ep_of(side, t, *at(here, step)), t),
                device_id_type=MESH,
            )
            copy.start()
            if line:
                arrivals[p, step] = copy

    def all_of(blocks, n):
        span = whole.at[pl.ds(0, blocks)]
        return pltpu.make_async_remote_copy(
            src_ref=span,
            dst_ref=span,
            send_sem=send_sem.at[0],
            recv_sem=recv_sem.at[n],
            device_id=other_core(),
            device_id_type=MESH,
        )

    for p, (_, _, first) in enumerate(pieces):
        if first is not None:
            first()
        spread(p, nothing, plane + lines)
    if then is not None:
        then()
    for offset in lines:
        for p in range(len(pieces)):
            arrivals[p, offset].wait_recv()
            spread(p, offset, plane)
    for offset in [nothing] + lines:
        all_of(len(plane), grouped + offset[0]).wait_recv()
        if landed is not None:
            landed(offset[0])

    return lambda: all_of(count - 1, 0).wait_send()


def contract(left, right):
    return lax.dot_general(left, right, (((1,), (1,)), ((), ())), preferred_element_type=FULL)


def dot(left, right):
    return jnp.dot(left, right, preferred_element_type=FULL)


def flat_rows(ref):
    blocks, rows, width = ref.shape
    return ref[...].astype(FULL).reshape(blocks * rows, width)


def grid_ids(*shape):
    return tuple(lax.broadcasted_iota(jnp.int32, shape, i) for i in range(2))


def sigmoid(v):
    return 1.0 / (1.0 + jnp.exp(-v))


def layer_kernel(count, names, pairs, *refs):
    r = types.SimpleNamespace(**dict(zip(names, refs)))
    for name in pairs:
        setattr(r, name, (getattr(r, name + "_send"), getattr(r, name + "_recv")))
    ep = lax.axis_index("ep")
    depth, side, t, *here = place(count)
    z, b, a = here
    lines, plane = peers_of(count)
    partner = (ep, 1 - t)
    own_rows, width = r.tokens.shape
    seqs = 2 * own_rows
    total = count * own_rows
    per = r.wq_hbm.shape[0]
    wide = 4 * per
    heads = r.beta.shape[0]
    part = per // heads
    size = width // (2 * heads)
    half = heads * size
    cols = r.wo.shape[2]
    my_slot = slot_of(depth, side, *here)
    slots = lambda ref: lambda z, b, a: ref.at[slot_of(depth, side, z, b, a)]

    loads = {}

    def load(name, src, dst):
        copy = pltpu.make_async_copy(src, dst, r.load_sem.at[len(loads)])
        copy.start()
        loads[name] = copy

    small = ("tokens", "gain", "beta", "decay", "rate", "bias", "head_gain")
    late = ("moe_gain", "mix", "ids", "route")
    for name in small:
        load(name, getattr(r, name + "_hbm"), getattr(r, name))
    projections = (r.wq_hbm, r.wk_hbm, r.wv_hbm, r.wz_hbm)
    spot_of = lambda p: r.weights.at[t, pl.ds(p * per, per)]
    for p, src in enumerate(projections):
        load(("w", p), src, spot_of(p))
    load("state", r.state_hbm, r.state)
    for name in late:
        load(name, getattr(r, name + "_hbm"), getattr(r, name))
    early, later = ("wo", "dg", "du", "eg"), ("eu", "dd", "ed")
    shards = early + later
    for name in shards:
        load(name, getattr(r, name + "_hbm"), getattr(r, name).at[t])

    barrier = pltpu.get_barrier_semaphore()
    devices = [partner] + [(ep_of(side, t, *at(here, o)), t) for o in plane + lines]
    for device in devices:
        pl.semaphore_signal(barrier, inc=1, device_id=device, device_id_type=MESH)
    loads["tokens"].wait()
    r.rows[my_slot] = r.tokens[...]
    r.pair[t] = r.tokens[...]
    pl.semaphore_wait(barrier, len(devices))

    crossed = {}

    def cross(name, src, dst):
        copy = remote(src, dst, r.core, len(crossed), partner)
        copy.start()
        crossed[name] = copy

    def order_ready():
        source, target = grid_ids(wide, wide)
        inner = source % per
        spot = inner % part * (4 * heads) + source // per * heads + inner // part
        r.order[...] = jnp.where(target == spot, 1.0, 0.0).astype(NARROW)

    def begin():
        cross("pair", r.tokens, r.pair.at[t])
        for p, src in enumerate(projections):
            cross(("w", p), src, spot_of(p))
        for name in early:
            cross(name, getattr(r, name + "_hbm"), getattr(r, name).at[t])
        order_ready()

    loads["gain"].wait()
    gain = r.gain[...]
    square = side * side

    def normalise(i):
        far = flip(z, i)
        for k in range(0, square, 2):
            first = far * square + k
            two = [r.rows[first + j].astype(FULL) for j in range(2)]
            two = rms_scale(jnp.concatenate(two, axis=0), gain).astype(NARROW)
            start = pl.multiple_of(first * own_rows, 2 * own_rows)
            r.normed[pl.ds(start, 2 * own_rows)] = two
        if i == 0:
            for p in range(4):
                loads["w", p].wait()
                crossed["w", p].wait_recv()
            order = r.order[...]
            for h in range(2):
                r.ordered[h] = lax.dot_general(
                    r.weights[h],
                    order,
                    (((0,), (0,)), ((), ())),
                    preferred_element_type=FULL,
                ).astype(NARROW)

    finish1 = gather(
        count, [(r.tokens, slots(r.rows), None)], r.ring1, r.rows, normalise, then=begin
    )
    left = r.normed[...]
    for h in range(2):
        product = dot(left, r.ordered[h])
        r.blocks[h] = product.reshape(count, own_rows, wide).astype(NARROW)

    for offset in [(i, j, k) for i in range(depth) for j in range(side) for k in range(side)][::-1]:
        z2, b2, a2 = at(here, offset)
        other = ep_of(side, t, z2, b2, a2)
        row = slot_of(depth, side, z2, b2, a2)
        for core in (1 - t, t):
            if offset == (0, 0, 0) and core is t:
                continue
            remote(
                r.blocks.at[core, row], r.landed.at[2 * ep + t], r.swap, 0, (other, core)
            ).start()
    r.landed[2 * ep + t] = r.blocks[t, my_slot]
    most = r.landed.at[pl.ds(0, 2 * count - 1)]
    exchange = remote(most, most, r.swap, 0, partner)

    if cols % 128 == 0:
        span = pl.ds(pl.multiple_of(ep * cols, 128), cols)
        r.columns[...] = r.rows[:, :, span].astype(FULL).reshape(total, cols)
    else:
        line, lane = grid_ids(width, cols)
        one = jnp.where(line == lane + ep * cols, 1.0, 0.0).astype(NARROW)
        r.columns[...] = dot(flat_rows(r.rows).astype(NARROW), one)
    crossed["pair"].wait_recv()
    for name in small[2:]:
        loads[name].wait()
    seq = rms_scale(flat_rows(r.pair), gain).astype(NARROW)
    line, lane = grid_ids(heads, heads)
    tall = lambda v: jnp.sum(jnp.where(line == lane, v, 0.0), axis=1, keepdims=True)
    beta = sigmoid(contract(r.beta[...], seq))
    pre = contract(r.decay[...], seq) + tall(r.bias[...])
    soft = jnp.maximum(pre, 0.0) + jnp.log1p(jnp.exp(-jnp.abs(pre)))
    retain = jnp.exp(-tall(r.rate[...]) * soft)
    for s in range(seqs):
        r.ready[4, s] = jnp.broadcast_to(beta[:, s : s + 1], (heads, size))
        r.ready[5, s] = jnp.broadcast_to(retain[:, s : s + 1], (heads, size))
    for name in late:
        loads[name].wait()
    weight = jnp.sum(jnp.where(r.ids[...] == ep, r.route[...], 0.0), axis=0, keepdims=True)
    line, lane = grid_ids(total, weight.shape[1])
    place_id = line // own_rows
    chip = ep_of(side, t, place_id // square, place_id % side, (place_id // side) % side)
    token = chip * seqs + t * own_rows + line % own_rows
    weight = jnp.sum(jnp.where(token == lane, weight, 0.0), axis=1, keepdims=True)
    r.weight[...] = jnp.broadcast_to(weight, r.weight.shape)
    r.mixes[...] = r.mix[...].astype(FULL)
    finish1()
    loads["state"].wait()
    exchange.wait()

    lanes = 4 * heads
    bunch = 128 // lanes
    arrived = r.landed[...].astype(FULL).reshape(count * seqs, wide)
    planes = r.flat.shape[0]
    for q in range(planes):
        span = arrived[:, q * 128 : (q + 1) * 128]
        r.flat[q, :, : span.shape[1]] = span
    for g in range(seqs // bunch):
        each = [
            [r.flat[q, pl.ds(g * bunch + s, count, stride=seqs), :] for q in range(planes)]
            for s in range(bunch)
        ]
        for j in range(part):
            q, i = j // bunch, j % bunch
            piece = [v[q][:, i * lanes : (i + 1) * lanes] for v in each]
            r.turned[g, pl.ds(j, count, stride=part), :] = jnp.concatenate(piece, axis=1)
    for g in range(seqs // bunch):
        split = silu(jnp.transpose(r.turned[g])).reshape(bunch, 4, heads, size)
        for p in range(4):
            v = split[:, p]
            if p < 2:
                v = v * lax.rsqrt(jnp.sum(v * v, axis=-1, keepdims=True) + EPS)
            if p == 0:
                v = v * size ** (-0.5)
            r.ready[p, g * bunch : (g + 1) * bunch] = v

    there = slot_of(depth, side, *place_of(count, ep, 1 - t))
    mine = pl.ds(pl.multiple_of(t * half, half), half)
    head_gain = r.head_gain[...]
    line = lax.broadcasted_iota(jnp.int32, (2 * heads, size), 0) % heads

    def readouts(core):
        first = core * own_rows
        reads = []
        for i in range(own_rows):
            s = first + i
            both = jnp.concatenate([r.ready[0, s], r.ready[1, s]], axis=0)
            high = both.astype(NARROW)
            low = (both - high.astype(FULL)).astype(NARROW)
            pushed = jnp.concatenate([high, low], axis=0)
            kept = jnp.zeros((2 * heads, size), FULL)
            for h in range(heads):
                got = dot(pushed, r.state[s, h].astype(NARROW))
                kept = jnp.where(line == h, got[: 2 * heads] + got[2 * heads :], kept)
            reads.append(kept)
        rows = pl.ds(pl.multiple_of(first, own_rows), own_rows)
        query, key, value, gate, beta, keep = (
            r.ready[p, rows].reshape(own_rows * heads, size) for p in range(6)
        )
        recalled = jnp.concatenate([v[heads:] for v in reads], axis=0)
        asked = jnp.concatenate([v[:heads] for v in reads], axis=0)
        write = beta * (value - keep * recalled)
        readout = keep * asked + jnp.sum(key * query, axis=1, keepdims=True) * write
        r.write[rows] = write.reshape(own_rows, heads, size)
        r.acc[...] = rms_scale(readout, head_gain) * gate
        for h in range(heads):
            piece = r.acc[pl.ds(h, own_rows, stride=heads), :]
            r.gated[core, :, h * size : (h + 1) * size] = piece.astype(NARROW)

    readouts(1 - t)
    swap = remote(
        r.gated.at[1 - t], r.mixed.at[there, :, mine], r.core, 5 + len(shards), partner
    )
    swap.start()
    for name in later:
        cross(name, getattr(r, name + "_hbm"), getattr(r, name).at[t])
    readouts(t)
    r.mixed[my_slot, :, mine] = r.gated[t]

    groups = seqs // bunch
    stores = [
        pltpu.make_async_copy(r.packed.at[span], r.pack.at[span], r.store_sem.at[i])
        for i, span in enumerate((pl.ds(0, 2 * groups + 2), pl.ds(2 * groups + 2, 1)))
    ]

    def prepare():
        keep = r.ready[5].reshape(seqs * heads, size)
        r.packed[2 * groups] = keep.astype(NARROW)
        r.packed[2 * groups + 1] = (keep - keep.astype(NARROW).astype(FULL)).astype(NARROW)
        none = jnp.zeros((heads, size), FULL)
        high = lambda v: v.astype(NARROW).astype(FULL)
        for g in range(groups):
            tall, across = [], []
            for s in range(g * bunch, (g + 1) * bunch):
                key, write = r.ready[1, s], r.write[s]
                tall += [high(key), high(key), key - high(key), none]
                across += [high(write), write - high(write), high(write), none]
            r.packed[g] = jnp.transpose(jnp.concatenate(tall, axis=0)).astype(NARROW)
            r.packed[groups + g] = jnp.concatenate(across, axis=0).astype(NARROW)
        stores[0].start()

    others = pl.ds(pl.multiple_of((1 - t) * half, half), half)
    part_of = lambda span: lambda z, b, a: r.mixed.at[slot_of(depth, side, z, b, a), :, span]
    came = r.mixed.at[my_slot, :, others]
    finish2 = gather(
        count,
        [(r.gated.at[t], part_of(mine), None), (came, part_of(others), swap.wait_recv)],
        r.ring2,
        r.mixed,
        then=prepare,
    )
    loads["wo"].wait()
    crossed["wo"].wait_recv()
    flat = flat_rows(r.mixed).astype(NARROW)
    resid = r.columns[...] + dot(flat[:, :half], r.wo[0]) + dot(flat[:, half:], r.wo[1])
    r.own[...] = (resid * r.moe_gain[pl.ds(ep, 1), :]).astype(NARROW)
    r.every[ep] = r.own[...]
    for name in ("dg", "du", "eg", "eu"):
        loads[name].wait()
        crossed[name].wait_recv()

    r.squares[...] = jnp.zeros_like(r.squares)
    r.logits[...] = jnp.zeros_like(r.logits)
    ffe = r.eg.shape[2]
    ffd = r.dg.shape[2]

    def absorb(i):
        far = flip(z, i)
        blocks = [r.every[far * square + k] for k in range(square)]
        squares, logits = r.squares[...], r.logits[...]
        for k, v in enumerate(blocks):
            v = v.astype(FULL)
            u = v / r.moe_gain[pl.ds(far * square + k, 1), :]
            squares = squares + u * u
            logits = logits + v * r.mixes[pl.ds(far * square + k, 1), :]
        r.squares[...], r.logits[...] = squares, logits
        left = jnp.concatenate(blocks, axis=1)
        span = pl.ds(pl.multiple_of(far * (square * cols), square * cols), square * cols)
        for dense, expert, low, high in (
            (r.dg, r.eg, r.dgate, r.egate),
            (r.du, r.eu, r.dup, r.eup),
        ):
            pair = jnp.concatenate([dense[0, span, :], dense[1, span, :]], axis=1)
            terms = [(low, 0, pair), (high, 0, expert[0, span, :]), (high, ffe, expert[1, span, :])]
            for ref, start, right in terms:
                lane = slice(start, start + right.shape[1])
                got = dot(left, right)
                if i:
                    got = got + ref[:, lane]
                ref[:, lane] = got

    finish3 = gather(
        count,
        [(r.own, lambda z, b, a: r.every.at[ep_of(side, t, z, b, a)], None)],
        r.ring3,
        r.every,
        absorb,
    )
    scale = jnp.sum(r.squares[...], axis=1, keepdims=True) * (1.0 / width)
    scale = lax.rsqrt(scale + EPS)
    dense_mix = sigmoid(scale * jnp.sum(r.logits[...], axis=1, keepdims=True))
    weight = r.weight[:, :1]
    for gate, up, act, factor in (
        (r.dgate, r.dup, r.dact, dense_mix),
        (r.egate, r.eup, r.eact, weight),
    ):
        step = min(256, act.shape[1])
        for start in range(0, act.shape[1], step):
            lane = slice(start, start + step)
            value = silu(scale * gate[:, lane]) * (scale * up[:, lane] * factor)
            act[:, lane] = value.astype(NARROW)
    for name in ("dd", "ed"):
        loads[name].wait()
        crossed[name].wait_recv()

    chunks, step = r.part.shape[0], r.part.shape[-1]

    def send(src, dst, offset, kind, c):
        pltpu.make_async_remote_copy(
            src_ref=src,
            dst_ref=dst,
            send_sem=r.reduce[0].at[kind],
            recv_sem=r.reduce[1].at[kind * chunks + c],
            device_id=(ep_of(side, t, *at(here, offset)), t),
            device_id_type=MESH,
        ).start()

    def arrived_all(ref, kind, c):
        pltpu.make_async_remote_copy(
            src_ref=ref,
            dst_ref=ref,
            send_sem=r.reduce[0].at[kind],
            recv_sem=r.reduce[1].at[kind * chunks + c],
            device_id=partner,
            device_id_type=MESH,
        ).wait_recv()

    def sent_all(ref, kind):
        pltpu.make_async_remote_copy(
            src_ref=ref,
            dst_ref=ref,
            send_sem=r.reduce[0].at[kind],
            recv_sem=r.reduce[1].at[0],
            device_id=partner,
            device_id_type=MESH,
        ).wait_send()

    for c in range(chunks):
        span = slice(c * step, (c + 1) * step)
        dense = r.dd[:, :, span].reshape(2 * ffd, step)
        expert = r.ed[:, :, span].reshape(2 * ffe, step)
        term = dot(r.dact[...], dense) + dot(r.eact[...], expert)
        r.part[c] = term.reshape(r.part.shape[1:]).astype(NARROW)
        for n, offset in enumerate(plane):
            _, b2, a2 = at(here, offset)
            send(r.part.at[c, :, a2, b2], r.plane_buf.at[c, n], offset, 0, c)
    line, lane = grid_ids(own_rows, total)
    pick = jnp.where(lane == line + my_slot * own_rows, 1.0, 0.0).astype(NARROW)
    for e in range(count):
        span = slice(e * cols, (e + 1) * cols)
        r.resid[:, span] = dot(pick, r.every[e]) / r.moe_gain[e : e + 1, :]
    for c in range(chunks):
        sums = r.part[c, :, a, b].astype(FULL)
        arrived_all(r.plane_buf.at[c], 0, c)
        for n in range(len(plane)):
            sums = sums + r.plane_buf[c, n].astype(FULL)
        r.sums[c] = sums.astype(NARROW)
        for n, offset in enumerate(lines):
            send(r.sums.at[c, flip(z, offset[0])], r.line_buf.at[c, n], offset, 1, c)
    for c in range(chunks):
        span = slice(c * step, (c + 1) * step)
        sums = r.resid[:, span] + r.sums[c, z].astype(FULL)
        arrived_all(r.line_buf.at[c], 1, c)
        for n in range(len(lines)):
            sums = sums + r.line_buf[c, n].astype(FULL)
        for k in range(0, step, 256):
            two = [sums[:, k + j : k + j + 128] for j in (0, 128)]
            first_row = (c * step + k) // 128 * own_rows
            rows = slice(first_row, first_row + 2 * own_rows)
            r.packed[2 * groups + 2, rows] = jnp.concatenate(two, axis=0).astype(NARROW)
    stores[1].start()
    stores[0].wait()
    for finish in (finish2, finish3, swap.wait_send):
        finish()
    for copy in crossed.values():
        copy.wait_send()
    sent_all(r.plane_buf, 0)
    sent_all(r.line_buf, 1)
    stores[1].wait()


def update_kernel(groups, pack_ref, state_ref, new_ref, out_ref, keeps):
    bunch, heads, size = state_ref.shape[:3]
    step = pl.program_id(0)

    @pl.when(step == 0)
    def _():
        keeps[...] = pack_ref[2 * groups].astype(FULL) + pack_ref[2 * groups + 1].astype(FULL)
        own_rows, width = out_ref.shape
        for e in range(width // 128):
            rows = pack_ref[2 * groups + 2, e * own_rows : (e + 1) * own_rows]
            out_ref[:, e * 128 : (e + 1) * 128] = rows

    tall = pack_ref[step]
    across = pack_ref[groups + step].astype(FULL)
    rank = 4 * heads
    row = lax.broadcasted_iota(jnp.int32, (rank, size), 0) % heads
    for s in range(bunch):
        left = tall[:, s * rank : (s + 1) * rank]
        right = across[s * rank : (s + 1) * rank]
        first = pl.multiple_of((step * bunch + s) * heads, heads)
        keep = keeps[pl.ds(first, heads)]
        for h in range(0, heads, 2):
            two = [jnp.where(row == h + i, right, 0.0) for i in range(2)]
            outer = dot(left, jnp.concatenate(two, axis=1).astype(NARROW))
            for i in range(2):
                kept = keep[h + i : h + i + 1] * state_ref[s, h + i]
                new_ref[s, h + i] = kept + outer[:, i * size : (i + 1) * size]


def update(groups, pack, state, layer):
    seqs, heads, size, _ = state.shape
    bunch = seqs // groups
    own = pl.BlockSpec((bunch, heads, size, size), lambda s: (s, 0, 0, 0))
    return pl.pallas_call(
        functools.partial(update_kernel, groups),
        grid=(seqs // bunch,),
        out_shape=(jax.ShapeDtypeStruct(state.shape, state.dtype), layer),
        in_specs=[pl.BlockSpec(pack.shape, lambda s: (0, 0, 0)), own],
        out_specs=(own, pl.BlockSpec(layer.shape, lambda s: (0, 0))),
        scratch_shapes=[VMEM((seqs * heads, size), FULL)],
        compiler_params=pltpu.CompilerParams(
            dimension_semantics=("arbitrary",), vmem_limit_bytes=16 * 1024 * 1024
        ),
        name="update",
    )(pack, state)


def body(
    tokens,
    mix_gain,
    w_query,
    w_key,
    w_value,
    w_zgate,
    w_beta,
    w_decay,
    decay_rate,
    decay_bias,
    head_gain,
    state,
    w_out,
    moe_gain,
    dense_mix,
    dense_gate,
    dense_up,
    dense_down,
    expert_gate,
    expert_up,
    expert_down,
    expert_ids,
    route_weight,
):
    count = lax.axis_size("ep")
    own_rows, width = tokens.shape
    seqs, heads, size, _ = state.shape
    depth, side = grid_of(count)
    total = count * own_rows
    flatten = lambda w: w.transpose(1, 2, 0).reshape(-1, width)
    cols = w_out.shape[1]
    operands = {
        "tokens": tokens,
        "gain": mix_gain.reshape(1, width),
        "beta": w_beta.T,
        "decay": w_decay.T,
        "rate": decay_rate.reshape(1, heads),
        "bias": decay_bias.reshape(1, heads),
        "head_gain": head_gain.reshape(1, size),
        "moe_gain": moe_gain.reshape(count, cols),
        "mix": dense_mix.reshape(count, cols),
        "ids": expert_ids.T,
        "route": route_weight.T,
    }
    split = {
        "wo": w_out,
        "dg": dense_gate,
        "du": dense_up,
        "dd": dense_down,
        "eg": expert_gate[0],
        "eu": expert_up[0],
        "ed": expert_down[0],
    }
    only = {
        "wq": flatten(w_query),
        "wk": flatten(w_key),
        "wv": flatten(w_value),
        "wz": flatten(w_zgate),
        "state": state,
    }
    wide = 4 * only["wq"].shape[0]
    ffd, ffe = dense_gate.shape[1], expert_gate.shape[2]
    chunks = 4
    room = 55 * 1024 if total * width <= 2**18 else 60 * 1024
    step = width // chunks
    group = 128 // (4 * heads)
    near, flat = side * side - 1, depth - 1
    narrow = lambda *shape: VMEM(shape, NARROW)
    full = lambda *shape: VMEM(shape, FULL)
    scratch = {k: VMEM(v.shape, v.dtype) for k, v in operands.items()}
    scratch |= {k: narrow(2, *v.shape) for k, v in split.items()}
    scratch |= {
        "state": full(*state.shape),
        "rows": narrow(count, own_rows, width),
        "pair": narrow(2, own_rows, width),
        "normed": narrow(total, width),
        "weights": narrow(2, wide, width),
        "order": narrow(wide, wide),
        "ordered": narrow(2, width, wide),
        "blocks": narrow(2, count, own_rows, wide),
        "landed": narrow(2 * count, own_rows, wide),
        "flat": full(-(-wide // 128), count * seqs, 128),
        "turned": full(seqs // group, size, 128),
        "columns": full(total, cols),
        "weight": full(total, 128),
        "mixes": full(count, cols),
        "ready": full(6, seqs, heads, size),
        "write": full(seqs, heads, size),
        "acc": full(own_rows * heads, size),
        "gated": narrow(2, own_rows, heads * size),
        "mixed": narrow(count, own_rows, width),
        "own": narrow(total, cols),
        "every": narrow(count, total, cols),
        "squares": full(total, cols),
        "logits": full(total, cols),
        "dgate": full(total, 2 * ffd),
        "dup": full(total, 2 * ffd),
        "egate": full(total, 2 * ffe),
        "eup": full(total, 2 * ffe),
        "dact": narrow(total, 2 * ffd),
        "eact": narrow(total, 2 * ffe),
        "part": narrow(chunks, depth, side, side, own_rows, step),
        "plane_buf": narrow(chunks, max(near, 1), depth, own_rows, step),
        "sums": narrow(chunks, depth, own_rows, step),
        "line_buf": narrow(chunks, max(flat, 1), own_rows, step),
        "resid": full(own_rows, width),
        "packed": narrow(2 * (seqs // group) + 3, 128, 128),
        "store_sem": pltpu.SemaphoreType.DMA((2,)),
        "load_sem": pltpu.SemaphoreType.DMA((len(operands) + len(split) + 5,)),
    }
    pairs = {
        "core": (6 + len(split), 6 + len(split)),
        "ring1": (1, 2 * depth - 1),
        "ring2": (1, 3 * depth - 2),
        "ring3": (1, 2 * depth - 1),
        "swap": (1, 1),
        "reduce": (2, 2 * chunks),
    }
    for name, (n, m) in pairs.items():
        scratch[name + "_send"] = pltpu.SemaphoreType.DMA((n,))
        scratch[name + "_recv"] = pltpu.SemaphoreType.DMA((m,))
    sources = operands | split | only
    outs = {"pack": jax.ShapeDtypeStruct((2 * (seqs // group) + 3, 128, 128), NARROW)}
    names = [k + "_hbm" for k in sources] + list(outs) + list(scratch)
    spec = pl.BlockSpec(memory_space=HBM)
    pack = pl.pallas_call(
        functools.partial(layer_kernel, count, names, tuple(pairs)),
        out_shape=outs["pack"],
        in_specs=[spec] * len(sources),
        out_specs=spec,
        scratch_shapes=list(scratch.values()),
        compiler_params=pltpu.CompilerParams(
            collective_id=1, has_side_effects=True, vmem_limit_bytes=room * 1024
        ),
        cost_estimate=pl.CostEstimate(
            flops=4 * 10**10, bytes_accessed=10**8, transcendentals=0
        ),
        name="layer",
    )(*sources.values())
    layer = jax.ShapeDtypeStruct((own_rows, width), NARROW)
    new_state, layer_out = update(seqs // group, pack, state, layer)
    return (layer_out, new_state)


def solution(mesh):
    placed = (
        P(("ep", "tp"), None),
        P(),
        P(None, "tp", "ep"),
        P(None, "tp", "ep"),
        P(None, "tp", "ep"),
        P(None, "tp", "ep"),
        P(None, "tp"),
        P(None, "tp"),
        P("tp"),
        P("tp"),
        P(),
        P("ep", "tp", None, None),
        P("tp", "ep"),
        P(),
        P(),
        P(None, ("ep", "tp")),
        P(None, ("ep", "tp")),
        P(("ep", "tp"), None),
        P("ep", None, "tp"),
        P("ep", None, "tp"),
        P("ep", "tp", None),
        P(),
        P(),
    )
    return jax.shard_map(
        body,
        mesh=mesh,
        in_specs=placed,
        out_specs=(P(("ep", "tp"), None), P("ep", "tp", None, None)),
        check_vma=False,
    )
```

```python
import functools
import types

import jax
import jax.numpy as jnp
from jax import lax
from jax.experimental import pallas as pl
from jax.experimental.pallas import tpu as pltpu
from jax.sharding import PartitionSpec as P

EPS = 1e-06
VMEM = pltpu.VMEM
HBM = pltpu.HBM
MESH = pl.DeviceIdType.MESH
NARROW, FULL = jnp.bfloat16, jnp.float32
TURNED = (3,)


def rms_scale(values, gain):
    return values * lax.rsqrt(jnp.mean(values * values, axis=-1, keepdims=True) + EPS) * gain


def silu(v):
    return v / (1.0 + jnp.exp(-v))


def grid_of(count):
    for depth in (4, 2, 1):
        side = int(round((count / depth) ** 0.5))
        if depth * side * side == count:
            return depth, side
    return count, 1


def place_of(count, ep, t):
    depth, side = grid_of(count)
    z = ep // (side * side)
    y = (ep // side) % side
    x = ep % side
    a = x * (1 - t) + y * t
    b = y * (1 - t) + x * t
    return z, b, a


def place(count):
    depth, side = grid_of(count)
    t = lax.axis_index("tp")
    z, b, a = place_of(count, lax.axis_index("ep"), t)
    return depth, side, t, z, b, a


def ep_of(side, t, z, b, a):
    y = b * (1 - t) + a * t
    x = a * (1 - t) + b * t
    return (z * side + y) * side + x


def slot_of(depth, side, z, b, a):
    return (z * side + a) * side + b


def flip(v, i):
    out = v
    bit = 1
    while bit <= i:
        if i & bit:
            out = out + bit - 2 * bit * ((v // bit) % 2)
        bit *= 2
    return out


def other_core():
    return (lax.axis_index("ep"), 1 - lax.axis_index("tp"))


def peers_of(count):
    depth, side = grid_of(count)
    plane = [(0, j, i) for j in range(side) for i in range(side)][1:]
    plane.sort(key=lambda o: -(o[1] > 0) - (o[2] > 0))
    return [(i, 0, 0) for i in range(1, depth)], plane


def at(here, offset):
    return tuple(flip(v, i) for v, i in zip(here, offset))


def plus(u, v):
    return tuple(i ^ j for i, j in zip(u, v))


def remote(src, dst, sems, n, device):
    return pltpu.make_async_remote_copy(
        src_ref=src,
        dst_ref=dst,
        send_sem=sems[0].at[n],
        recv_sem=sems[1].at[n],
        device_id=device,
        device_id_type=MESH,
    )


def gather(count, pieces, sems, whole, landed=None, then=None):
    depth, side, t, *here = place(count)
    lines, plane = peers_of(count)
    straight = [o for o in plane if not (o[1] and o[2])]
    corner = [o for o in plane if o[1] and o[2]]
    turned = [o for o in lines if o[0] in TURNED]
    nothing = (0, 0, 0)
    send_sem, recv_sem = sems
    grouped = len(pieces) * len(lines)
    alone = grouped + depth

    def spread(p, offset, steps):
        source, view, _ = pieces[p]
        spot = view(*at(here, offset))
        for step in steps:
            to = plus(offset, step)
            if to in lines:
                n = p * len(lines) + to[0] - 1
            elif to in corner:
                n = alone + p * len(corner) + corner.index(to)
            else:
                n = grouped + to[0]
            pltpu.make_async_remote_copy(
                src_ref=source if offset == nothing else spot,
                dst_ref=spot,
                send_sem=send_sem.at[0],
                recv_sem=recv_sem.at[n],
                device_id=(ep_of(side, t, *at(here, step)), t),
                device_id_type=MESH,
            ).start()

    def wait(span, n):
        return pltpu.make_async_remote_copy(
            src_ref=span,
            dst_ref=span,
            send_sem=send_sem.at[0],
            recv_sem=recv_sem.at[n],
            device_id=other_core(),
            device_id_type=MESH,
        )

    def pass_on(p, offset, n, steps):
        wait(pieces[p][1](*at(here, offset)), n).wait_recv()
        spread(p, offset, steps)

    for p, (_, _, first) in enumerate(pieces):
        if first is not None:
            first()
        spread(p, nothing, plane + lines)
    if then is not None:
        then()
    for i, offset in enumerate(lines):
        for p in range(len(pieces)):
            steps = straight if offset in turned else plane
            pass_on(p, offset, p * len(lines) + offset[0] - 1, steps)
        if i == 0:
            for p in range(len(pieces)):
                for k, far in enumerate(corner):
                    pass_on(p, far, alone + p * len(corner) + k, turned)
    for offset in [nothing] + lines:
        blocks = len(straight) if offset == nothing else len(plane)
        wait(whole.at[pl.ds(0, blocks)], grouped + offset[0]).wait_recv()
        if landed is not None:
            landed(offset[0])

    whole_send = wait(whole.at[pl.ds(0, count - 1)], 0)
    return whole_send.wait_send


def contract(left, right):
    return lax.dot_general(left, right, (((1,), (1,)), ((), ())), preferred_element_type=FULL)


def dot(left, right):
    return jnp.dot(left, right, preferred_element_type=FULL)


def flat_rows(ref):
    blocks, rows, width = ref.shape
    return ref[...].astype(FULL).reshape(blocks * rows, width)


def grid_ids(*shape):
    return tuple(lax.broadcasted_iota(jnp.int32, shape, i) for i in range(2))


def sigmoid(v):
    return 1.0 / (1.0 + jnp.exp(-v))


def layer_kernel(count, names, pairs, *refs):
    r = types.SimpleNamespace(**dict(zip(names, refs)))
    for name in pairs:
        setattr(r, name, (getattr(r, name + "_send"), getattr(r, name + "_recv")))
    ep = lax.axis_index("ep")
    depth, side, t, *here = place(count)
    z, b, a = here
    lines, plane = peers_of(count)
    partner = (ep, 1 - t)
    own_rows, width = r.tokens.shape
    seqs = 2 * own_rows
    total = count * own_rows
    per = r.wq_hbm.shape[0]
    wide = 4 * per
    heads = r.beta.shape[0]
    part = per // heads
    size = width // (2 * heads)
    half = heads * size
    cols = r.wo.shape[2]
    my_slot = slot_of(depth, side, *here)
    slots = lambda ref: lambda z, b, a: ref.at[slot_of(depth, side, z, b, a)]

    loads = {}

    def load(name, src, dst):
        copy = pltpu.make_async_copy(src, dst, r.load_sem.at[len(loads)])
        copy.start()
        loads[name] = copy

    small = ("tokens", "gain", "beta", "decay", "rate", "bias", "head_gain")
    late = ("moe_gain", "mix", "ids", "route")
    for name in small:
        load(name, getattr(r, name + "_hbm"), getattr(r, name))
    projections = (r.wq_hbm, r.wk_hbm, r.wv_hbm, r.wz_hbm)
    spot_of = lambda p: r.weights.at[t, pl.ds(p * per, per)]
    for p, src in enumerate(projections):
        load(("w", p), src, spot_of(p))
    load("state", r.state_hbm, r.state)
    for name in late:
        load(name, getattr(r, name + "_hbm"), getattr(r, name))
    early, later = ("wo", "dg", "du", "eg"), ("eu", "dd", "ed")
    shards = early + later
    for name in shards:
        load(name, getattr(r, name + "_hbm"), getattr(r, name).at[t])

    barrier = pltpu.get_barrier_semaphore()
    devices = [partner] + [(ep_of(side, t, *at(here, o)), t) for o in plane + lines]
    for device in devices:
        pl.semaphore_signal(barrier, inc=1, device_id=device, device_id_type=MESH)
    loads["tokens"].wait()
    r.rows[my_slot] = r.tokens[...]
    r.pair[t] = r.tokens[...]
    pl.semaphore_wait(barrier, len(devices))

    crossed = {}

    def cross(name, src, dst):
        copy = remote(src, dst, r.core, len(crossed), partner)
        copy.start()
        crossed[name] = copy

    def order_ready():
        source, target = grid_ids(wide, wide)
        inner = source % per
        spot = inner % part * (4 * heads) + source // per * heads + inner // part
        r.order[...] = jnp.where(target == spot, 1.0, 0.0).astype(NARROW)

    def begin():
        cross("pair", r.tokens, r.pair.at[t])
        for p, src in enumerate(projections):
            cross(("w", p), src, spot_of(p))
        for name in early:
            cross(name, getattr(r, name + "_hbm"), getattr(r, name).at[t])
        order_ready()

    loads["gain"].wait()
    gain = r.gain[...]
    square = side * side

    def normalise(i):
        far = flip(z, i)
        for k in range(0, square, 2):
            first = far * square + k
            two = [r.rows[first + j].astype(FULL) for j in range(2)]
            two = rms_scale(jnp.concatenate(two, axis=0), gain).astype(NARROW)
            start = pl.multiple_of(first * own_rows, 2 * own_rows)
            r.normed[pl.ds(start, 2 * own_rows)] = two
        if i == 0:
            for p in range(4):
                loads["w", p].wait()
                crossed["w", p].wait_recv()
            order = r.order[...]
            for h in range(2):
                r.ordered[h] = lax.dot_general(
                    r.weights[h],
                    order,
                    (((0,), (0,)), ((), ())),
                    preferred_element_type=FULL,
                ).astype(NARROW)

    finish1 = gather(
        count, [(r.tokens, slots(r.rows), None)], r.ring1, r.rows, normalise, then=begin
    )
    left = r.normed[...]
    for h in range(2):
        product = dot(left, r.ordered[h])
        r.blocks[h] = product.reshape(count, own_rows, wide).astype(NARROW)

    for offset in [(i, j, k) for i in range(depth) for j in range(side) for k in range(side)][::-1]:
        z2, b2, a2 = at(here, offset)
        other = ep_of(side, t, z2, b2, a2)
        row = slot_of(depth, side, z2, b2, a2)
        for core in (1 - t, t):
            if offset == (0, 0, 0) and core is t:
                continue
            remote(
                r.blocks.at[core, row], r.landed.at[2 * ep + t], r.swap, 0, (other, core)
            ).start()
    r.landed[2 * ep + t] = r.blocks[t, my_slot]
    most = r.landed.at[pl.ds(0, 2 * count - 1)]
    exchange = remote(most, most, r.swap, 0, partner)

    if cols % 128 == 0:
        span = pl.ds(pl.multiple_of(ep * cols, 128), cols)
        r.columns[...] = r.rows[:, :, span].astype(FULL).reshape(total, cols)
    else:
        line, lane = grid_ids(width, cols)
        one = jnp.where(line == lane + ep * cols, 1.0, 0.0).astype(NARROW)
        r.columns[...] = dot(flat_rows(r.rows).astype(NARROW), one)
    crossed["pair"].wait_recv()
    for name in small[2:]:
        loads[name].wait()
    seq = rms_scale(flat_rows(r.pair), gain).astype(NARROW)
    line, lane = grid_ids(heads, heads)
    tall = lambda v: jnp.sum(jnp.where(line == lane, v, 0.0), axis=1, keepdims=True)
    beta = sigmoid(contract(r.beta[...], seq))
    pre = contract(r.decay[...], seq) + tall(r.bias[...])
    soft = jnp.maximum(pre, 0.0) + jnp.log1p(jnp.exp(-jnp.abs(pre)))
    retain = jnp.exp(-tall(r.rate[...]) * soft)
    for s in range(seqs):
        r.ready[4, s] = jnp.broadcast_to(beta[:, s : s + 1], (heads, size))
        r.ready[5, s] = jnp.broadcast_to(retain[:, s : s + 1], (heads, size))
    for name in late:
        loads[name].wait()
    weight = jnp.sum(jnp.where(r.ids[...] == ep, r.route[...], 0.0), axis=0, keepdims=True)
    line, lane = grid_ids(total, weight.shape[1])
    place_id = line // own_rows
    chip = ep_of(side, t, place_id // square, place_id % side, (place_id // side) % side)
    token = chip * seqs + t * own_rows + line % own_rows
    weight = jnp.sum(jnp.where(token == lane, weight, 0.0), axis=1, keepdims=True)
    r.weight[...] = jnp.broadcast_to(weight, r.weight.shape)
    r.mixes[...] = r.mix[...].astype(FULL)
    finish1()
    loads["state"].wait()
    exchange.wait()

    lanes = 4 * heads
    bunch = 128 // lanes
    arrived = r.landed[...].astype(FULL).reshape(count * seqs, wide)
    planes = r.flat.shape[0]
    for q in range(planes):
        span = arrived[:, q * 128 : (q + 1) * 128]
        r.flat[q, :, : span.shape[1]] = span
    for g in range(seqs // bunch):
        each = [
            [r.flat[q, pl.ds(g * bunch + s, count, stride=seqs), :] for q in range(planes)]
            for s in range(bunch)
        ]
        for j in range(part):
            q, i = j // bunch, j % bunch
            piece = [v[q][:, i * lanes : (i + 1) * lanes] for v in each]
            r.turned[g, pl.ds(j, count, stride=part), :] = jnp.concatenate(piece, axis=1)
    for g in range(seqs // bunch):
        split = silu(jnp.transpose(r.turned[g])).reshape(bunch, 4, heads, size)
        for p in range(4):
            v = split[:, p]
            if p < 2:
                v = v * lax.rsqrt(jnp.sum(v * v, axis=-1, keepdims=True) + EPS)
            if p == 0:
                v = v * size ** (-0.5)
            r.ready[p, g * bunch : (g + 1) * bunch] = v

    there = slot_of(depth, side, *place_of(count, ep, 1 - t))
    mine = pl.ds(pl.multiple_of(t * half, half), half)
    head_gain = r.head_gain[...]
    line = lax.broadcasted_iota(jnp.int32, (2 * heads, size), 0) % heads

    def readouts(core):
        first = core * own_rows
        reads = []
        for i in range(own_rows):
            s = first + i
            both = jnp.concatenate([r.ready[0, s], r.ready[1, s]], axis=0)
            high = both.astype(NARROW)
            low = (both - high.astype(FULL)).astype(NARROW)
            pushed = jnp.concatenate([high, low], axis=0)
            kept = jnp.zeros((2 * heads, size), FULL)
            for h in range(heads):
                got = dot(pushed, r.state[s, h].astype(NARROW))
                kept = jnp.where(line == h, got[: 2 * heads] + got[2 * heads :], kept)
            reads.append(kept)
        rows = pl.ds(pl.multiple_of(first, own_rows), own_rows)
        query, key, value, gate, beta, keep = (
            r.ready[p, rows].reshape(own_rows * heads, size) for p in range(6)
        )
        recalled = jnp.concatenate([v[heads:] for v in reads], axis=0)
        asked = jnp.concatenate([v[:heads] for v in reads], axis=0)
        write = beta * (value - keep * recalled)
        readout = keep * asked + jnp.sum(key * query, axis=1, keepdims=True) * write
        r.write[rows] = write.reshape(own_rows, heads, size)
        r.acc[...] = rms_scale(readout, head_gain) * gate
        for h in range(heads):
            piece = r.acc[pl.ds(h, own_rows, stride=heads), :]
            r.gated[core, :, h * size : (h + 1) * size] = piece.astype(NARROW)

    readouts(1 - t)
    swap = remote(
        r.gated.at[1 - t], r.mixed.at[there, :, mine], r.core, 5 + len(shards), partner
    )
    swap.start()
    for name in later:
        cross(name, getattr(r, name + "_hbm"), getattr(r, name).at[t])
    readouts(t)
    r.mixed[my_slot, :, mine] = r.gated[t]

    groups = seqs // bunch
    stores = [
        pltpu.make_async_copy(r.packed.at[span], r.pack.at[span], r.store_sem.at[i])
        for i, span in enumerate((pl.ds(0, 2 * groups + 2), pl.ds(2 * groups + 2, 1)))
    ]

    def prepare():
        keep = r.ready[5].reshape(seqs * heads, size)
        r.packed[2 * groups] = keep.astype(NARROW)
        r.packed[2 * groups + 1] = (keep - keep.astype(NARROW).astype(FULL)).astype(NARROW)
        none = jnp.zeros((heads, size), FULL)
        high = lambda v: v.astype(NARROW).astype(FULL)
        for g in range(groups):
            tall, across = [], []
            for s in range(g * bunch, (g + 1) * bunch):
                key, write = r.ready[1, s], r.write[s]
                tall += [high(key), high(key), key - high(key), none]
                across += [high(write), write - high(write), high(write), none]
            r.packed[g] = jnp.transpose(jnp.concatenate(tall, axis=0)).astype(NARROW)
            r.packed[groups + g] = jnp.concatenate(across, axis=0).astype(NARROW)
        stores[0].start()

    others = pl.ds(pl.multiple_of((1 - t) * half, half), half)
    part_of = lambda span: lambda z, b, a: r.mixed.at[slot_of(depth, side, z, b, a), :, span]
    came = r.mixed.at[my_slot, :, others]
    finish2 = gather(
        count,
        [(r.gated.at[t], part_of(mine), None), (came, part_of(others), swap.wait_recv)],
        r.ring2,
        r.mixed,
        then=prepare,
    )
    loads["wo"].wait()
    crossed["wo"].wait_recv()
    flat = flat_rows(r.mixed).astype(NARROW)
    resid = r.columns[...] + dot(flat[:, :half], r.wo[0]) + dot(flat[:, half:], r.wo[1])
    r.own[...] = (resid * r.moe_gain[pl.ds(ep, 1), :]).astype(NARROW)
    r.every[ep] = r.own[...]
    for name in ("dg", "du", "eg", "eu"):
        loads[name].wait()
        crossed[name].wait_recv()

    r.squares[...] = jnp.zeros_like(r.squares)
    r.logits[...] = jnp.zeros_like(r.logits)
    ffe = r.eg.shape[2]
    ffd = r.dg.shape[2]

    def absorb(i):
        far = flip(z, i)
        blocks = [r.every[far * square + k] for k in range(square)]
        squares, logits = r.squares[...], r.logits[...]
        for k, v in enumerate(blocks):
            v = v.astype(FULL)
            u = v / r.moe_gain[pl.ds(far * square + k, 1), :]
            squares = squares + u * u
            logits = logits + v * r.mixes[pl.ds(far * square + k, 1), :]
        r.squares[...], r.logits[...] = squares, logits
        left = jnp.concatenate(blocks, axis=1)
        span = pl.ds(pl.multiple_of(far * (square * cols), square * cols), square * cols)
        for dense, expert, low, high in (
            (r.dg, r.eg, r.dgate, r.egate),
            (r.du, r.eu, r.dup, r.eup),
        ):
            pair = jnp.concatenate([dense[0, span, :], dense[1, span, :]], axis=1)
            terms = [(low, 0, pair), (high, 0, expert[0, span, :]), (high, ffe, expert[1, span, :])]
            for ref, start, right in terms:
                lane = slice(start, start + right.shape[1])
                got = dot(left, right)
                if i:
                    got = got + ref[:, lane]
                ref[:, lane] = got

    finish3 = gather(
        count,
        [(r.own, lambda z, b, a: r.every.at[ep_of(side, t, z, b, a)], None)],
        r.ring3,
        r.every,
        absorb,
    )
    scale = jnp.sum(r.squares[...], axis=1, keepdims=True) * (1.0 / width)
    scale = lax.rsqrt(scale + EPS)
    dense_mix = sigmoid(scale * jnp.sum(r.logits[...], axis=1, keepdims=True))
    weight = r.weight[:, :1]
    for gate, up, act, factor in (
        (r.dgate, r.dup, r.dact, dense_mix),
        (r.egate, r.eup, r.eact, weight),
    ):
        step = min(256, act.shape[1])
        for start in range(0, act.shape[1], step):
            lane = slice(start, start + step)
            value = silu(scale * gate[:, lane]) * (scale * up[:, lane] * factor)
            act[:, lane] = value.astype(NARROW)
    for name in ("dd", "ed"):
        loads[name].wait()
        crossed[name].wait_recv()

    chunks, step = r.part.shape[0], r.part.shape[-1]

    def send(src, dst, offset, kind, c):
        pltpu.make_async_remote_copy(
            src_ref=src,
            dst_ref=dst,
            send_sem=r.reduce[0].at[kind],
            recv_sem=r.reduce[1].at[kind * chunks + c],
            device_id=(ep_of(side, t, *at(here, offset)), t),
            device_id_type=MESH,
        ).start()

    def arrived_all(ref, kind, c):
        pltpu.make_async_remote_copy(
            src_ref=ref,
            dst_ref=ref,
            send_sem=r.reduce[0].at[kind],
            recv_sem=r.reduce[1].at[kind * chunks + c],
            device_id=partner,
            device_id_type=MESH,
        ).wait_recv()

    def sent_all(ref, kind):
        pltpu.make_async_remote_copy(
            src_ref=ref,
            dst_ref=ref,
            send_sem=r.reduce[0].at[kind],
            recv_sem=r.reduce[1].at[0],
            device_id=partner,
            device_id_type=MESH,
        ).wait_send()

    for c in range(chunks):
        span = slice(c * step, (c + 1) * step)
        dense = r.dd[:, :, span].reshape(2 * ffd, step)
        expert = r.ed[:, :, span].reshape(2 * ffe, step)
        term = dot(r.dact[...], dense) + dot(r.eact[...], expert)
        r.part[c] = term.reshape(r.part.shape[1:]).astype(NARROW)
        for n, offset in enumerate(plane):
            _, b2, a2 = at(here, offset)
            send(r.part.at[c, :, a2, b2], r.plane_buf.at[c, n], offset, 0, c)
    line, lane = grid_ids(own_rows, total)
    pick = jnp.where(lane == line + my_slot * own_rows, 1.0, 0.0).astype(NARROW)
    for e in range(count):
        span = slice(e * cols, (e + 1) * cols)
        r.resid[:, span] = dot(pick, r.every[e]) / r.moe_gain[e : e + 1, :]
    for c in range(chunks):
        sums = r.part[c, :, a, b].astype(FULL)
        arrived_all(r.plane_buf.at[c], 0, c)
        for n in range(len(plane)):
            sums = sums + r.plane_buf[c, n].astype(FULL)
        r.sums[c] = sums.astype(NARROW)
        for n, offset in enumerate(lines):
            send(r.sums.at[c, flip(z, offset[0])], r.line_buf.at[c, n], offset, 1, c)
    for c in range(chunks):
        span = slice(c * step, (c + 1) * step)
        sums = r.resid[:, span] + r.sums[c, z].astype(FULL)
        arrived_all(r.line_buf.at[c], 1, c)
        for n in range(len(lines)):
            sums = sums + r.line_buf[c, n].astype(FULL)
        for k in range(0, step, 256):
            two = [sums[:, k + j : k + j + 128] for j in (0, 128)]
            first_row = (c * step + k) // 128 * own_rows
            rows = slice(first_row, first_row + 2 * own_rows)
            r.packed[2 * groups + 2, rows] = jnp.concatenate(two, axis=0).astype(NARROW)
    stores[1].start()
    stores[0].wait()
    for finish in (finish2, finish3, swap.wait_send):
        finish()
    for copy in crossed.values():
        copy.wait_send()
    sent_all(r.plane_buf, 0)
    sent_all(r.line_buf, 1)
    stores[1].wait()


def update_kernel(groups, pack_ref, state_ref, new_ref, out_ref, keeps):
    bunch, heads, size = state_ref.shape[:3]
    step = pl.program_id(0)

    @pl.when(step == 0)
    def _():
        keeps[...] = pack_ref[2 * groups].astype(FULL) + pack_ref[2 * groups + 1].astype(FULL)
        own_rows, width = out_ref.shape
        for e in range(width // 128):
            rows = pack_ref[2 * groups + 2, e * own_rows : (e + 1) * own_rows]
            out_ref[:, e * 128 : (e + 1) * 128] = rows

    tall = pack_ref[step]
    across = pack_ref[groups + step].astype(FULL)
    rank = 4 * heads
    row = lax.broadcasted_iota(jnp.int32, (rank, size), 0) % heads
    for s in range(bunch):
        left = tall[:, s * rank : (s + 1) * rank]
        right = across[s * rank : (s + 1) * rank]
        first = pl.multiple_of((step * bunch + s) * heads, heads)
        keep = keeps[pl.ds(first, heads)]
        for h in range(0, heads, 2):
            two = [jnp.where(row == h + i, right, 0.0) for i in range(2)]
            outer = dot(left, jnp.concatenate(two, axis=1).astype(NARROW))
            for i in range(2):
                kept = keep[h + i : h + i + 1] * state_ref[s, h + i]
                new_ref[s, h + i] = kept + outer[:, i * size : (i + 1) * size]


def update(groups, pack, state, layer):
    seqs, heads, size, _ = state.shape
    bunch = seqs // groups
    own = pl.BlockSpec((bunch, heads, size, size), lambda s: (s, 0, 0, 0))
    return pl.pallas_call(
        functools.partial(update_kernel, groups),
        grid=(seqs // bunch,),
        out_shape=(jax.ShapeDtypeStruct(state.shape, state.dtype), layer),
        in_specs=[pl.BlockSpec(pack.shape, lambda s: (0, 0, 0)), own],
        out_specs=(own, pl.BlockSpec(layer.shape, lambda s: (0, 0))),
        scratch_shapes=[VMEM((seqs * heads, size), FULL)],
        compiler_params=pltpu.CompilerParams(
            dimension_semantics=("arbitrary",), vmem_limit_bytes=16 * 1024 * 1024
        ),
        name="update",
    )(pack, state)


def body(
    tokens,
    mix_gain,
    w_query,
    w_key,
    w_value,
    w_zgate,
    w_beta,
    w_decay,
    decay_rate,
    decay_bias,
    head_gain,
    state,
    w_out,
    moe_gain,
    dense_mix,
    dense_gate,
    dense_up,
    dense_down,
    expert_gate,
    expert_up,
    expert_down,
    expert_ids,
    route_weight,
):
    count = lax.axis_size("ep")
    own_rows, width = tokens.shape
    seqs, heads, size, _ = state.shape
    depth, side = grid_of(count)
    total = count * own_rows
    flatten = lambda w: w.transpose(1, 2, 0).reshape(-1, width)
    cols = w_out.shape[1]
    operands = {
        "tokens": tokens,
        "gain": mix_gain.reshape(1, width),
        "beta": w_beta.T,
        "decay": w_decay.T,
        "rate": decay_rate.reshape(1, heads),
        "bias": decay_bias.reshape(1, heads),
        "head_gain": head_gain.reshape(1, size),
        "moe_gain": moe_gain.reshape(count, cols),
        "mix": dense_mix.reshape(count, cols),
        "ids": expert_ids.T,
        "route": route_weight.T,
    }
    split = {
        "wo": w_out,
        "dg": dense_gate,
        "du": dense_up,
        "dd": dense_down,
        "eg": expert_gate[0],
        "eu": expert_up[0],
        "ed": expert_down[0],
    }
    only = {
        "wq": flatten(w_query),
        "wk": flatten(w_key),
        "wv": flatten(w_value),
        "wz": flatten(w_zgate),
        "state": state,
    }
    wide = 4 * only["wq"].shape[0]
    ffd, ffe = dense_gate.shape[1], expert_gate.shape[2]
    chunks = 4
    room = 55 * 1024 if total * width <= 2**18 else 60 * 1024
    step = width // chunks
    group = 128 // (4 * heads)
    near, flat = side * side - 1, depth - 1
    corners = (side - 1) ** 2
    narrow = lambda *shape: VMEM(shape, NARROW)
    full = lambda *shape: VMEM(shape, FULL)
    scratch = {k: VMEM(v.shape, v.dtype) for k, v in operands.items()}
    scratch |= {k: narrow(2, *v.shape) for k, v in split.items()}
    scratch |= {
        "state": full(*state.shape),
        "rows": narrow(count, own_rows, width),
        "pair": narrow(2, own_rows, width),
        "normed": narrow(total, width),
        "weights": narrow(2, wide, width),
        "order": narrow(wide, wide),
        "ordered": narrow(2, width, wide),
        "blocks": narrow(2, count, own_rows, wide),
        "landed": narrow(2 * count, own_rows, wide),
        "flat": full(-(-wide // 128), count * seqs, 128),
        "turned": full(seqs // group, size, 128),
        "columns": full(total, cols),
        "weight": full(total, 128),
        "mixes": full(count, cols),
        "ready": full(6, seqs, heads, size),
        "write": full(seqs, heads, size),
        "acc": full(own_rows * heads, size),
        "gated": narrow(2, own_rows, heads * size),
        "mixed": narrow(count, own_rows, width),
        "own": narrow(total, cols),
        "every": narrow(count, total, cols),
        "squares": full(total, cols),
        "logits": full(total, cols),
        "dgate": full(total, 2 * ffd),
        "dup": full(total, 2 * ffd),
        "egate": full(total, 2 * ffe),
        "eup": full(total, 2 * ffe),
        "dact": narrow(total, 2 * ffd),
        "eact": narrow(total, 2 * ffe),
        "part": narrow(chunks, depth, side, side, own_rows, step),
        "plane_buf": narrow(chunks, max(near, 1), depth, own_rows, step),
        "sums": narrow(chunks, depth, own_rows, step),
        "line_buf": narrow(chunks, max(flat, 1), own_rows, step),
        "resid": full(own_rows, width),
        "packed": narrow(2 * (seqs // group) + 3, 128, 128),
        "store_sem": pltpu.SemaphoreType.DMA((2,)),
        "load_sem": pltpu.SemaphoreType.DMA((len(operands) + len(split) + 5,)),
    }
    pairs = {
        "core": (6 + len(split), 6 + len(split)),
        "ring1": (1, 2 * depth - 1 + corners),
        "ring2": (1, 3 * depth - 2 + 2 * corners),
        "ring3": (1, 2 * depth - 1 + corners),
        "swap": (1, 1),
        "reduce": (2, 2 * chunks),
    }
    for name, (n, m) in pairs.items():
        scratch[name + "_send"] = pltpu.SemaphoreType.DMA((n,))
        scratch[name + "_recv"] = pltpu.SemaphoreType.DMA((m,))
    sources = operands | split | only
    outs = {"pack": jax.ShapeDtypeStruct((2 * (seqs // group) + 3, 128, 128), NARROW)}
    names = [k + "_hbm" for k in sources] + list(outs) + list(scratch)
    spec = pl.BlockSpec(memory_space=HBM)
    pack = pl.pallas_call(
        functools.partial(layer_kernel, count, names, tuple(pairs)),
        out_shape=outs["pack"],
        in_specs=[spec] * len(sources),
        out_specs=spec,
        scratch_shapes=list(scratch.values()),
        compiler_params=pltpu.CompilerParams(
            collective_id=1, has_side_effects=True, vmem_limit_bytes=room * 1024
        ),
        cost_estimate=pl.CostEstimate(
            flops=4 * 10**10, bytes_accessed=10**8, transcendentals=0
        ),
        name="layer",
    )(*sources.values())
    layer = jax.ShapeDtypeStruct((own_rows, width), NARROW)
    new_state, layer_out = update(seqs // group, pack, state, layer)
    return (layer_out, new_state)


def solution(mesh):
    placed = (
        P(("ep", "tp"), None),
        P(),
        P(None, "tp", "ep"),
        P(None, "tp", "ep"),
        P(None, "tp", "ep"),
        P(None, "tp", "ep"),
        P(None, "tp"),
        P(None, "tp"),
        P("tp"),
        P("tp"),
        P(),
        P("ep", "tp", None, None),
        P("tp", "ep"),
        P(),
        P(),
        P(None, ("ep", "tp")),
        P(None, ("ep", "tp")),
        P(("ep", "tp"), None),
        P("ep", None, "tp"),
        P("ep", None, "tp"),
        P("ep", "tp", None),
        P(),
        P(),
    )
    return jax.shard_map(
        body,
        mesh=mesh,
        in_specs=placed,
        out_specs=(P(("ep", "tp"), None), P("ep", "tp", None, None)),
        check_vma=False,
    )
```

```python
import functools
import types

import jax
import jax.numpy as jnp
from jax import lax
from jax.experimental import pallas as pl
from jax.experimental.pallas import tpu as pltpu
from jax.sharding import PartitionSpec as P

EPS = 1e-06
VMEM = pltpu.VMEM
HBM = pltpu.HBM
MESH = pl.DeviceIdType.MESH
NARROW, FULL = jnp.bfloat16, jnp.float32
TURNED = (3,)


def rms_scale(values, gain):
    return values * lax.rsqrt(jnp.mean(values * values, axis=-1, keepdims=True) + EPS) * gain


def silu(v):
    return v / (1.0 + jnp.exp(-v))


def grid_of(count):
    for depth in (4, 2, 1):
        side = int(round((count / depth) ** 0.5))
        if depth * side * side == count:
            return depth, side
    return count, 1


def place_of(count, ep, t):
    depth, side = grid_of(count)
    z = ep // (side * side)
    y = (ep // side) % side
    x = ep % side
    a = x * (1 - t) + y * t
    b = y * (1 - t) + x * t
    return z, b, a


def place(count):
    depth, side = grid_of(count)
    t = lax.axis_index("tp")
    z, b, a = place_of(count, lax.axis_index("ep"), t)
    return depth, side, t, z, b, a


def ep_of(side, t, z, b, a):
    y = b * (1 - t) + a * t
    x = a * (1 - t) + b * t
    return (z * side + y) * side + x


def slot_of(depth, side, z, b, a):
    return (z * side + a) * side + b


def flip(v, i):
    out = v
    bit = 1
    while bit <= i:
        if i & bit:
            out = out + bit - 2 * bit * ((v // bit) % 2)
        bit *= 2
    return out


def other_core():
    return (lax.axis_index("ep"), 1 - lax.axis_index("tp"))


def peers_of(count):
    depth, side = grid_of(count)
    plane = [(0, j, i) for j in range(side) for i in range(side)][1:]
    plane.sort(key=lambda o: -(o[1] > 0) - (o[2] > 0))
    return [(i, 0, 0) for i in range(1, depth)], plane


def at(here, offset):
    return tuple(flip(v, i) for v, i in zip(here, offset))


def plus(u, v):
    return tuple(i ^ j for i, j in zip(u, v))


def remote(src, dst, sems, n, device):
    return pltpu.make_async_remote_copy(
        src_ref=src,
        dst_ref=dst,
        send_sem=sems[0].at[n],
        recv_sem=sems[1].at[n],
        device_id=device,
        device_id_type=MESH,
    )


def gather(count, pieces, sems, whole, landed=None, then=None):
    depth, side, t, *here = place(count)
    lines, plane = peers_of(count)
    straight = [o for o in plane if not (o[1] and o[2])]
    corner = [o for o in plane if o[1] and o[2]]
    turned = [o for o in lines if o[0] in TURNED]
    nothing = (0, 0, 0)
    send_sem, recv_sem = sems
    grouped = len(pieces) * len(lines)
    alone = grouped + depth

    def spread(p, offset, steps):
        source, view, _ = pieces[p]
        spot = view(*at(here, offset))
        for step in steps:
            to = plus(offset, step)
            if to in lines:
                n = p * len(lines) + to[0] - 1
            elif to in corner:
                n = alone + p * len(corner) + corner.index(to)
            else:
                n = grouped + to[0]
            pltpu.make_async_remote_copy(
                src_ref=source if offset == nothing else spot,
                dst_ref=spot,
                send_sem=send_sem.at[0],
                recv_sem=recv_sem.at[n],
                device_id=(ep_of(side, t, *at(here, step)), t),
                device_id_type=MESH,
            ).start()

    def wait(span, n):
        return pltpu.make_async_remote_copy(
            src_ref=span,
            dst_ref=span,
            send_sem=send_sem.at[0],
            recv_sem=recv_sem.at[n],
            device_id=other_core(),
            device_id_type=MESH,
        )

    def pass_on(p, offset, n, steps):
        wait(pieces[p][1](*at(here, offset)), n).wait_recv()
        spread(p, offset, steps)

    for p, (_, _, first) in enumerate(pieces):
        if first is not None:
            first()
        spread(p, nothing, plane + lines)
    if then is not None:
        then()
    for i, offset in enumerate(lines):
        for p in range(len(pieces)):
            steps = straight if offset in turned else plane
            pass_on(p, offset, p * len(lines) + offset[0] - 1, steps)
        if i == 0:
            for p in range(len(pieces)):
                for k, far in enumerate(corner):
                    pass_on(p, far, alone + p * len(corner) + k, turned)
    for offset in [nothing] + lines:
        blocks = len(straight) if offset == nothing else len(plane)
        wait(whole.at[pl.ds(0, blocks)], grouped + offset[0]).wait_recv()
        if landed is not None:
            landed(offset[0])

    whole_send = wait(whole.at[pl.ds(0, count - 1)], 0)
    return whole_send.wait_send


def contract(left, right):
    return lax.dot_general(left, right, (((1,), (1,)), ((), ())), preferred_element_type=FULL)


def dot(left, right):
    return jnp.dot(left, right, preferred_element_type=FULL)


def flat_rows(ref):
    blocks, rows, width = ref.shape
    return ref[...].astype(FULL).reshape(blocks * rows, width)


def grid_ids(*shape):
    return tuple(lax.broadcasted_iota(jnp.int32, shape, i) for i in range(2))


def sigmoid(v):
    return 1.0 / (1.0 + jnp.exp(-v))


def layer_kernel(count, names, pairs, *refs):
    r = types.SimpleNamespace(**dict(zip(names, refs)))
    for name in pairs:
        setattr(r, name, (getattr(r, name + "_send"), getattr(r, name + "_recv")))
    ep = lax.axis_index("ep")
    depth, side, t, *here = place(count)
    z, b, a = here
    lines, plane = peers_of(count)
    partner = (ep, 1 - t)
    own_rows, width = r.tokens.shape
    seqs = 2 * own_rows
    total = count * own_rows
    per = r.wq_hbm.shape[0]
    wide = 4 * per
    heads = r.beta.shape[0]
    part = per // heads
    size = width // (2 * heads)
    half = heads * size
    cols = r.wo.shape[2]
    my_slot = slot_of(depth, side, *here)
    slots = lambda ref: lambda z, b, a: ref.at[slot_of(depth, side, z, b, a)]

    loads = {}

    def load(name, src, dst):
        copy = pltpu.make_async_copy(src, dst, r.load_sem.at[len(loads)])
        copy.start()
        loads[name] = copy

    small = ("tokens", "gain", "beta", "decay", "rate", "bias", "head_gain")
    late = ("moe_gain", "mix", "ids", "route")
    for name in small:
        load(name, getattr(r, name + "_hbm"), getattr(r, name))
    projections = (r.wq_hbm, r.wk_hbm, r.wv_hbm, r.wz_hbm)
    spot_of = lambda p: r.weights.at[t, pl.ds(p * per, per)]
    for p, src in enumerate(projections):
        load(("w", p), src, spot_of(p))
    load("state", r.state_hbm, r.state)
    for name in late:
        load(name, getattr(r, name + "_hbm"), getattr(r, name))
    early, later = ("wo", "dg", "du", "eg"), ("eu", "dd", "ed")
    shards = early + later
    for name in shards:
        load(name, getattr(r, name + "_hbm"), getattr(r, name).at[t])

    barrier = pltpu.get_barrier_semaphore()
    devices = [partner] + [(ep_of(side, t, *at(here, o)), t) for o in plane + lines]
    for device in devices:
        pl.semaphore_signal(barrier, inc=1, device_id=device, device_id_type=MESH)
    loads["tokens"].wait()
    r.rows[my_slot] = r.tokens[...]
    r.pair[t] = r.tokens[...]
    pl.semaphore_wait(barrier, len(devices))

    crossed = {}

    def cross(name, src, dst):
        copy = remote(src, dst, r.core, len(crossed), partner)
        copy.start()
        crossed[name] = copy

    def order_ready():
        source, target = grid_ids(wide, wide)
        inner = source % per
        spot = inner % part * (4 * heads) + source // per * heads + inner // part
        r.order[...] = jnp.where(target == spot, 1.0, 0.0).astype(NARROW)

    def begin():
        cross("pair", r.tokens, r.pair.at[t])
        for p, src in enumerate(projections):
            cross(("w", p), src, spot_of(p))
        for name in early:
            cross(name, getattr(r, name + "_hbm"), getattr(r, name).at[t])
        order_ready()

    loads["gain"].wait()
    gain = r.gain[...]
    square = side * side

    def normalise(i):
        far = flip(z, i)
        for k in range(0, square, 2):
            first = far * square + k
            two = [r.rows[first + j].astype(FULL) for j in range(2)]
            two = rms_scale(jnp.concatenate(two, axis=0), gain).astype(NARROW)
            start = pl.multiple_of(first * own_rows, 2 * own_rows)
            r.normed[pl.ds(start, 2 * own_rows)] = two
        if i == 0:
            for p in range(4):
                loads["w", p].wait()
                crossed["w", p].wait_recv()
            order = r.order[...]
            for h in range(2):
                r.ordered[h] = lax.dot_general(
                    r.weights[h],
                    order,
                    (((0,), (0,)), ((), ())),
                    preferred_element_type=FULL,
                ).astype(NARROW)

    finish1 = gather(
        count, [(r.tokens, slots(r.rows), None)], r.ring1, r.rows, normalise, then=begin
    )
    left = r.normed[...]
    for h in range(2):
        product = dot(left, r.ordered[h])
        r.blocks[h] = product.reshape(count, own_rows, wide).astype(NARROW)

    for offset in [(i, j, k) for i in range(depth) for j in range(side) for k in range(side)][::-1]:
        z2, b2, a2 = at(here, offset)
        other = ep_of(side, t, z2, b2, a2)
        row = slot_of(depth, side, z2, b2, a2)
        for core in (1 - t, t):
            if offset == (0, 0, 0) and core is t:
                continue
            remote(
                r.blocks.at[core, row], r.landed.at[2 * ep + t], r.swap, 0, (other, core)
            ).start()
    r.landed[2 * ep + t] = r.blocks[t, my_slot]
    most = r.landed.at[pl.ds(0, 2 * count - 1)]
    exchange = remote(most, most, r.swap, 0, partner)

    if cols % 128 == 0:
        span = pl.ds(pl.multiple_of(ep * cols, 128), cols)
        r.columns[...] = r.rows[:, :, span].astype(FULL).reshape(total, cols)
    else:
        line, lane = grid_ids(width, cols)
        one = jnp.where(line == lane + ep * cols, 1.0, 0.0).astype(NARROW)
        r.columns[...] = dot(flat_rows(r.rows).astype(NARROW), one)
    crossed["pair"].wait_recv()
    for name in small[2:]:
        loads[name].wait()
    seq = rms_scale(flat_rows(r.pair), gain).astype(NARROW)
    line, lane = grid_ids(heads, heads)
    tall = lambda v: jnp.sum(jnp.where(line == lane, v, 0.0), axis=1, keepdims=True)
    beta = sigmoid(contract(r.beta[...], seq))
    pre = contract(r.decay[...], seq) + tall(r.bias[...])
    soft = jnp.maximum(pre, 0.0) + jnp.log1p(jnp.exp(-jnp.abs(pre)))
    retain = jnp.exp(-tall(r.rate[...]) * soft)
    for s in range(seqs):
        r.ready[4, s] = jnp.broadcast_to(beta[:, s : s + 1], (heads, size))
        r.ready[5, s] = jnp.broadcast_to(retain[:, s : s + 1], (heads, size))
    for name in late:
        loads[name].wait()
    weight = jnp.sum(jnp.where(r.ids[...] == ep, r.route[...], 0.0), axis=0, keepdims=True)
    line, lane = grid_ids(total, weight.shape[1])
    place_id = line // own_rows
    chip = ep_of(side, t, place_id // square, place_id % side, (place_id // side) % side)
    token = chip * seqs + t * own_rows + line % own_rows
    weight = jnp.sum(jnp.where(token == lane, weight, 0.0), axis=1, keepdims=True)
    r.weight[...] = jnp.broadcast_to(weight, r.weight.shape)
    r.mixes[...] = r.mix[...].astype(FULL)
    finish1()
    loads["state"].wait()
    exchange.wait()

    lanes = 4 * heads
    bunch = 128 // lanes
    arrived = r.landed[...].astype(FULL).reshape(count * seqs, wide)
    planes = r.flat.shape[0]
    for q in range(planes):
        span = arrived[:, q * 128 : (q + 1) * 128]
        r.flat[q, :, : span.shape[1]] = span
    for g in range(seqs // bunch):
        each = [
            [r.flat[q, pl.ds(g * bunch + s, count, stride=seqs), :] for q in range(planes)]
            for s in range(bunch)
        ]
        for j in range(part):
            q, i = j // bunch, j % bunch
            piece = [v[q][:, i * lanes : (i + 1) * lanes] for v in each]
            r.turned[g, pl.ds(j, count, stride=part), :] = jnp.concatenate(piece, axis=1)
    for g in range(seqs // bunch):
        split = silu(jnp.transpose(r.turned[g])).reshape(bunch, 4, heads, size)
        for p in range(4):
            v = split[:, p]
            if p < 2:
                v = v * lax.rsqrt(jnp.sum(v * v, axis=-1, keepdims=True) + EPS)
            if p == 0:
                v = v * size ** (-0.5)
            r.ready[p, g * bunch : (g + 1) * bunch] = v

    there = slot_of(depth, side, *place_of(count, ep, 1 - t))
    mine = pl.ds(pl.multiple_of(t * half, half), half)
    head_gain = r.head_gain[...]
    line = lax.broadcasted_iota(jnp.int32, (2 * heads, size), 0) % heads

    def readouts(core):
        first = core * own_rows
        reads = []
        for i in range(own_rows):
            s = first + i
            both = jnp.concatenate([r.ready[0, s], r.ready[1, s]], axis=0)
            high = both.astype(NARROW)
            low = (both - high.astype(FULL)).astype(NARROW)
            pushed = jnp.concatenate([high, low], axis=0)
            kept = jnp.zeros((2 * heads, size), FULL)
            for h in range(heads):
                got = dot(pushed, r.state[s, h].astype(NARROW))
                kept = jnp.where(line == h, got[: 2 * heads] + got[2 * heads :], kept)
            reads.append(kept)
        rows = pl.ds(pl.multiple_of(first, own_rows), own_rows)
        query, key, value, gate, beta, keep = (
            r.ready[p, rows].reshape(own_rows * heads, size) for p in range(6)
        )
        recalled = jnp.concatenate([v[heads:] for v in reads], axis=0)
        asked = jnp.concatenate([v[:heads] for v in reads], axis=0)
        write = beta * (value - keep * recalled)
        readout = keep * asked + jnp.sum(key * query, axis=1, keepdims=True) * write
        r.write[rows] = write.reshape(own_rows, heads, size)
        r.acc[...] = rms_scale(readout, head_gain) * gate
        for h in range(heads):
            piece = r.acc[pl.ds(h, own_rows, stride=heads), :]
            r.gated[core, :, h * size : (h + 1) * size] = piece.astype(NARROW)

    readouts(1 - t)
    swap = remote(
        r.gated.at[1 - t], r.mixed.at[there, :, mine], r.core, 5 + len(shards), partner
    )
    swap.start()
    for name in later:
        cross(name, getattr(r, name + "_hbm"), getattr(r, name).at[t])
    readouts(t)
    r.mixed[my_slot, :, mine] = r.gated[t]

    groups = seqs // bunch
    stores = [
        pltpu.make_async_copy(r.packed.at[span], r.pack.at[span], r.store_sem.at[i])
        for i, span in enumerate((pl.ds(0, 2 * groups + 2), pl.ds(2 * groups + 2, 1)))
    ]

    def prepare():
        keep = r.ready[5].reshape(seqs * heads, size)
        r.packed[2 * groups] = keep.astype(NARROW)
        r.packed[2 * groups + 1] = (keep - keep.astype(NARROW).astype(FULL)).astype(NARROW)
        none = jnp.zeros((heads, size), FULL)
        high = lambda v: v.astype(NARROW).astype(FULL)
        for g in range(groups):
            tall, across = [], []
            for s in range(g * bunch, (g + 1) * bunch):
                key, write = r.ready[1, s], r.write[s]
                tall += [high(key), high(key), key - high(key), none]
                across += [high(write), write - high(write), high(write), none]
            r.packed[g] = jnp.transpose(jnp.concatenate(tall, axis=0)).astype(NARROW)
            r.packed[groups + g] = jnp.concatenate(across, axis=0).astype(NARROW)
        stores[0].start()

    others = pl.ds(pl.multiple_of((1 - t) * half, half), half)
    part_of = lambda span: lambda z, b, a: r.mixed.at[slot_of(depth, side, z, b, a), :, span]
    came = r.mixed.at[my_slot, :, others]
    finish2 = gather(
        count,
        [(r.gated.at[t], part_of(mine), None), (came, part_of(others), swap.wait_recv)],
        r.ring2,
        r.mixed,
        then=prepare,
    )
    loads["wo"].wait()
    crossed["wo"].wait_recv()
    flat = flat_rows(r.mixed).astype(NARROW)
    resid = r.columns[...] + dot(flat[:, :half], r.wo[0]) + dot(flat[:, half:], r.wo[1])
    r.own[...] = (resid * r.moe_gain[pl.ds(ep, 1), :]).astype(NARROW)
    r.every[ep] = r.own[...]
    for name in ("dg", "du", "eg", "eu"):
        loads[name].wait()
        crossed[name].wait_recv()

    r.squares[...] = jnp.zeros_like(r.squares)
    r.logits[...] = jnp.zeros_like(r.logits)
    ffe = r.eg.shape[2]
    ffd = r.dg.shape[2]

    def absorb(i):
        far = flip(z, i)
        blocks = [r.every[far * square + k] for k in range(square)]
        squares, logits = r.squares[...], r.logits[...]
        for k, v in enumerate(blocks):
            v = v.astype(FULL)
            u = v / r.moe_gain[pl.ds(far * square + k, 1), :]
            squares = squares + u * u
            logits = logits + v * r.mixes[pl.ds(far * square + k, 1), :]
        r.squares[...], r.logits[...] = squares, logits
        left = jnp.concatenate(blocks, axis=1)
        span = pl.ds(pl.multiple_of(far * (square * cols), square * cols), square * cols)
        for dense, expert, low, high in (
            (r.dg, r.eg, r.dgate, r.egate),
            (r.du, r.eu, r.dup, r.eup),
        ):
            pair = jnp.concatenate([dense[0, span, :], dense[1, span, :]], axis=1)
            terms = [(low, 0, pair), (high, 0, expert[0, span, :]), (high, ffe, expert[1, span, :])]
            for ref, start, right in terms:
                lane = slice(start, start + right.shape[1])
                got = dot(left, right)
                if i:
                    got = got + ref[:, lane]
                ref[:, lane] = got

    finish3 = gather(
        count,
        [(r.own, lambda z, b, a: r.every.at[ep_of(side, t, z, b, a)], None)],
        r.ring3,
        r.every,
        absorb,
    )
    scale = jnp.sum(r.squares[...], axis=1, keepdims=True) * (1.0 / width)
    scale = lax.rsqrt(scale + EPS)
    dense_mix = sigmoid(scale * jnp.sum(r.logits[...], axis=1, keepdims=True))
    weight = r.weight[:, :1]
    for gate, up, act, factor in (
        (r.dgate, r.dup, r.dact, dense_mix),
        (r.egate, r.eup, r.eact, weight),
    ):
        step = min(256, act.shape[1])
        for start in range(0, act.shape[1], step):
            lane = slice(start, start + step)
            value = silu(scale * gate[:, lane]) * (scale * up[:, lane] * factor)
            act[:, lane] = value.astype(NARROW)
    for name in ("dd", "ed"):
        loads[name].wait()
        crossed[name].wait_recv()

    chunks, step = r.part.shape[0], r.part.shape[-1]

    def send(src, dst, offset, kind, c):
        pltpu.make_async_remote_copy(
            src_ref=src,
            dst_ref=dst,
            send_sem=r.reduce[0].at[kind],
            recv_sem=r.reduce[1].at[kind * chunks + c],
            device_id=(ep_of(side, t, *at(here, offset)), t),
            device_id_type=MESH,
        ).start()

    def arrived_all(ref, kind, c):
        pltpu.make_async_remote_copy(
            src_ref=ref,
            dst_ref=ref,
            send_sem=r.reduce[0].at[kind],
            recv_sem=r.reduce[1].at[kind * chunks + c],
            device_id=partner,
            device_id_type=MESH,
        ).wait_recv()

    def sent_all(ref, kind):
        pltpu.make_async_remote_copy(
            src_ref=ref,
            dst_ref=ref,
            send_sem=r.reduce[0].at[kind],
            recv_sem=r.reduce[1].at[0],
            device_id=partner,
            device_id_type=MESH,
        ).wait_send()

    for c in range(chunks):
        span = slice(c * step, (c + 1) * step)
        dense = r.dd[:, :, span].reshape(2 * ffd, step)
        expert = r.ed[:, :, span].reshape(2 * ffe, step)
        term = dot(r.dact[...], dense) + dot(r.eact[...], expert)
        r.part[c] = term.reshape(r.part.shape[1:]).astype(NARROW)
        for n, offset in enumerate(plane):
            _, b2, a2 = at(here, offset)
            send(r.part.at[c, :, a2, b2], r.plane_buf.at[c, n], offset, 0, c)
    line, lane = grid_ids(own_rows, total)
    pick = jnp.where(lane == line + my_slot * own_rows, 1.0, 0.0).astype(NARROW)
    for e in range(count):
        span = slice(e * cols, (e + 1) * cols)
        r.resid[:, span] = dot(pick, r.every[e]) / r.moe_gain[e : e + 1, :]
    for c in range(chunks):
        sums = r.part[c, :, a, b].astype(FULL)
        arrived_all(r.plane_buf.at[c], 0, c)
        for n in range(len(plane)):
            sums = sums + r.plane_buf[c, n].astype(FULL)
        r.sums[c] = sums.astype(NARROW)
        for n, offset in reversed(list(enumerate(lines))):
            send(r.sums.at[c, flip(z, offset[0])], r.line_buf.at[c, n], offset, 1, c)
    for c in range(chunks):
        span = slice(c * step, (c + 1) * step)
        sums = r.resid[:, span] + r.sums[c, z].astype(FULL)
        arrived_all(r.line_buf.at[c], 1, c)
        for n in range(len(lines)):
            sums = sums + r.line_buf[c, n].astype(FULL)
        for k in range(0, step, 256):
            two = [sums[:, k + j : k + j + 128] for j in (0, 128)]
            first_row = (c * step + k) // 128 * own_rows
            rows = slice(first_row, first_row + 2 * own_rows)
            r.packed[2 * groups + 2, rows] = jnp.concatenate(two, axis=0).astype(NARROW)
    stores[1].start()
    stores[0].wait()
    for finish in (finish2, finish3, swap.wait_send):
        finish()
    for copy in crossed.values():
        copy.wait_send()
    sent_all(r.plane_buf, 0)
    sent_all(r.line_buf, 1)
    stores[1].wait()


def update_kernel(groups, pack_ref, state_ref, new_ref, out_ref, keeps):
    bunch, heads, size = state_ref.shape[:3]
    step = pl.program_id(0)

    @pl.when(step == 0)
    def _():
        keeps[...] = pack_ref[2 * groups].astype(FULL) + pack_ref[2 * groups + 1].astype(FULL)
        own_rows, width = out_ref.shape
        for e in range(width // 128):
            rows = pack_ref[2 * groups + 2, e * own_rows : (e + 1) * own_rows]
            out_ref[:, e * 128 : (e + 1) * 128] = rows

    tall = pack_ref[step]
    across = pack_ref[groups + step].astype(FULL)
    rank = 4 * heads
    row = lax.broadcasted_iota(jnp.int32, (rank, size), 0) % heads
    for s in range(bunch):
        left = tall[:, s * rank : (s + 1) * rank]
        right = across[s * rank : (s + 1) * rank]
        first = pl.multiple_of((step * bunch + s) * heads, heads)
        keep = keeps[pl.ds(first, heads)]
        for h in range(0, heads, 2):
            two = [jnp.where(row == h + i, right, 0.0) for i in range(2)]
            outer = dot(left, jnp.concatenate(two, axis=1).astype(NARROW))
            for i in range(2):
                kept = keep[h + i : h + i + 1] * state_ref[s, h + i]
                new_ref[s, h + i] = kept + outer[:, i * size : (i + 1) * size]


def update(groups, pack, state, layer):
    seqs, heads, size, _ = state.shape
    bunch = seqs // groups
    own = pl.BlockSpec((bunch, heads, size, size), lambda s: (s, 0, 0, 0))
    return pl.pallas_call(
        functools.partial(update_kernel, groups),
        grid=(seqs // bunch,),
        out_shape=(jax.ShapeDtypeStruct(state.shape, state.dtype), layer),
        in_specs=[pl.BlockSpec(pack.shape, lambda s: (0, 0, 0)), own],
        out_specs=(own, pl.BlockSpec(layer.shape, lambda s: (0, 0))),
        scratch_shapes=[VMEM((seqs * heads, size), FULL)],
        compiler_params=pltpu.CompilerParams(
            dimension_semantics=("arbitrary",), vmem_limit_bytes=16 * 1024 * 1024
        ),
        name="update",
    )(pack, state)


def body(
    tokens,
    mix_gain,
    w_query,
    w_key,
    w_value,
    w_zgate,
    w_beta,
    w_decay,
    decay_rate,
    decay_bias,
    head_gain,
    state,
    w_out,
    moe_gain,
    dense_mix,
    dense_gate,
    dense_up,
    dense_down,
    expert_gate,
    expert_up,
    expert_down,
    expert_ids,
    route_weight,
):
    count = lax.axis_size("ep")
    own_rows, width = tokens.shape
    seqs, heads, size, _ = state.shape
    depth, side = grid_of(count)
    total = count * own_rows
    flatten = lambda w: w.transpose(1, 2, 0).reshape(-1, width)
    cols = w_out.shape[1]
    operands = {
        "tokens": tokens,
        "gain": mix_gain.reshape(1, width),
        "beta": w_beta.T,
        "decay": w_decay.T,
        "rate": decay_rate.reshape(1, heads),
        "bias": decay_bias.reshape(1, heads),
        "head_gain": head_gain.reshape(1, size),
        "moe_gain": moe_gain.reshape(count, cols),
        "mix": dense_mix.reshape(count, cols),
        "ids": expert_ids.T,
        "route": route_weight.T,
    }
    split = {
        "wo": w_out,
        "dg": dense_gate,
        "du": dense_up,
        "dd": dense_down,
        "eg": expert_gate[0],
        "eu": expert_up[0],
        "ed": expert_down[0],
    }
    only = {
        "wq": flatten(w_query),
        "wk": flatten(w_key),
        "wv": flatten(w_value),
        "wz": flatten(w_zgate),
        "state": state,
    }
    wide = 4 * only["wq"].shape[0]
    ffd, ffe = dense_gate.shape[1], expert_gate.shape[2]
    chunks = 4
    room = 55 * 1024 if total * width <= 2**18 else 60 * 1024
    step = width // chunks
    group = 128 // (4 * heads)
    near, flat = side * side - 1, depth - 1
    corners = (side - 1) ** 2
    narrow = lambda *shape: VMEM(shape, NARROW)
    full = lambda *shape: VMEM(shape, FULL)
    scratch = {k: VMEM(v.shape, v.dtype) for k, v in operands.items()}
    scratch |= {k: narrow(2, *v.shape) for k, v in split.items()}
    scratch |= {
        "state": full(*state.shape),
        "rows": narrow(count, own_rows, width),
        "pair": narrow(2, own_rows, width),
        "normed": narrow(total, width),
        "weights": narrow(2, wide, width),
        "order": narrow(wide, wide),
        "ordered": narrow(2, width, wide),
        "blocks": narrow(2, count, own_rows, wide),
        "landed": narrow(2 * count, own_rows, wide),
        "flat": full(-(-wide // 128), count * seqs, 128),
        "turned": full(seqs // group, size, 128),
        "columns": full(total, cols),
        "weight": full(total, 128),
        "mixes": full(count, cols),
        "ready": full(6, seqs, heads, size),
        "write": full(seqs, heads, size),
        "acc": full(own_rows * heads, size),
        "gated": narrow(2, own_rows, heads * size),
        "mixed": narrow(count, own_rows, width),
        "own": narrow(total, cols),
        "every": narrow(count, total, cols),
        "squares": full(total, cols),
        "logits": full(total, cols),
        "dgate": full(total, 2 * ffd),
        "dup": full(total, 2 * ffd),
        "egate": full(total, 2 * ffe),
        "eup": full(total, 2 * ffe),
        "dact": narrow(total, 2 * ffd),
        "eact": narrow(total, 2 * ffe),
        "part": narrow(chunks, depth, side, side, own_rows, step),
        "plane_buf": narrow(chunks, max(near, 1), depth, own_rows, step),
        "sums": narrow(chunks, depth, own_rows, step),
        "line_buf": narrow(chunks, max(flat, 1), own_rows, step),
        "resid": full(own_rows, width),
        "packed": narrow(2 * (seqs // group) + 3, 128, 128),
        "store_sem": pltpu.SemaphoreType.DMA((2,)),
        "load_sem": pltpu.SemaphoreType.DMA((len(operands) + len(split) + 5,)),
    }
    pairs = {
        "core": (6 + len(split), 6 + len(split)),
        "ring1": (1, 2 * depth - 1 + corners),
        "ring2": (1, 3 * depth - 2 + 2 * corners),
        "ring3": (1, 2 * depth - 1 + corners),
        "swap": (1, 1),
        "reduce": (2, 2 * chunks),
    }
    for name, (n, m) in pairs.items():
        scratch[name + "_send"] = pltpu.SemaphoreType.DMA((n,))
        scratch[name + "_recv"] = pltpu.SemaphoreType.DMA((m,))
    sources = operands | split | only
    outs = {"pack": jax.ShapeDtypeStruct((2 * (seqs // group) + 3, 128, 128), NARROW)}
    names = [k + "_hbm" for k in sources] + list(outs) + list(scratch)
    spec = pl.BlockSpec(memory_space=HBM)
    pack = pl.pallas_call(
        functools.partial(layer_kernel, count, names, tuple(pairs)),
        out_shape=outs["pack"],
        in_specs=[spec] * len(sources),
        out_specs=spec,
        scratch_shapes=list(scratch.values()),
        compiler_params=pltpu.CompilerParams(
            collective_id=1, has_side_effects=True, vmem_limit_bytes=room * 1024
        ),
        cost_estimate=pl.CostEstimate(
            flops=4 * 10**10, bytes_accessed=10**8, transcendentals=0
        ),
        name="layer",
    )(*sources.values())
    layer = jax.ShapeDtypeStruct((own_rows, width), NARROW)
    new_state, layer_out = update(seqs // group, pack, state, layer)
    return (layer_out, new_state)


def solution(mesh):
    placed = (
        P(("ep", "tp"), None),
        P(),
        P(None, "tp", "ep"),
        P(None, "tp", "ep"),
        P(None, "tp", "ep"),
        P(None, "tp", "ep"),
        P(None, "tp"),
        P(None, "tp"),
        P("tp"),
        P("tp"),
        P(),
        P("ep", "tp", None, None),
        P("tp", "ep"),
        P(),
        P(),
        P(None, ("ep", "tp")),
        P(None, ("ep", "tp")),
        P(("ep", "tp"), None),
        P("ep", None, "tp"),
        P("ep", None, "tp"),
        P("ep", "tp", None),
        P(),
        P(),
    )
    return jax.shard_map(
        body,
        mesh=mesh,
        in_specs=placed,
        out_specs=(P(("ep", "tp"), None), P("ep", "tp", None, None)),
        check_vma=False,
    )
```
